32 devices in a mesh: ep: 8 (over z, y), tp: 4 (over x, core).
Axes of the slice: x: 2, y: 2, z: 4, core: 2. Of those that a mesh axis runs over, the one named last changes fastest.
Arguments:
- att_queries: bfloat16 [8192, 1024], P(('ep', 'tp')), may hold values from -8 to 8
- att_keys: bfloat16 [8192, 256], P(('ep', 'tp')), may hold values from -6 to 6
- att_values: bfloat16 [8192, 256], P(('ep', 'tp')), may hold values from -6 to 6
- sink_logits: float32 [16], replicated, may hold values from 3 to 6.5
- out_weight: bfloat16 [1024, 2048], replicated, may hold values from -0.1875 to 0.1875
- att_gain: float32 [2048], replicated, may hold values from 0.1 to 1.9
- moe_in: bfloat16 [4096, 2048], P(('ep', 'tp')), may hold values from -6 to 6
- pre_gain: float32 [2048], replicated, may hold values from 0.1 to 1.9
- expert_ids: int32 [4096, 2], P(('ep', 'tp')), may hold values from 0 to 15, all different within a row; in each aligned block of 128 rows (0 to 127, 128 to 255, ...) at most 32 rows name the same one
- routed_expert_weight: float32 [4096, 2], P(('ep', 'tp')), may hold values from 0.2 to 1.5
- w_gate: bfloat16 [16, 2048, 768], P('ep', None, 'tp'), may hold values from -0.125 to 0.125
- w_up: bfloat16 [16, 2048, 768], P('ep', None, 'tp'), may hold values from -0.125 to 0.125
- w_down: bfloat16 [16, 768, 2048], P('ep', 'tp'), may hold values from -0.21875 to 0.21875
- common_expert_gate_weight: bfloat16 [2048, 512], P(None, 'tp'), may hold values from -0.125 to 0.125
- common_expert_up_weight: bfloat16 [2048, 512], P(None, 'tp'), may hold values from -0.125 to 0.125
- common_expert_down_weight: bfloat16 [512, 2048], P('tp'), may hold values from -0.25 to 0.25
- moe_gain: float32 [2048], replicated, may hold values from 0.1 to 1.9
Outputs:
- mixer_out: bfloat16 [8192, 2048], P(('ep', 'tp'))
- experts_out: bfloat16 [4096, 2048], P(('ep', 'tp'))
The draws below stay inside these ranges and needn't reach their ends.
Inputs may be any that keep to these rules, and one draw needn't show every extreme that they name: `expert_ids`: each row names 2 different experts; within the rows of one device no expert is named more than 32 times, and in every draw some expert is named exactly 32 times by the rows of some device.
All inputs are finite; a program needn't handle non-finite values.
Results may differ from the reference program's by a relative error of at most 0.012.
Values may be sent and summed in bfloat16 or wider, within the bound.
A program may use at most 128 MiB of HBM per device.

```python
import math
import jax
import jax.numpy as jnp
import numpy as np
from jax import lax

D = 2048
HEADS = 16
KV_HEADS = 4
HEAD_DIM = 64
WINDOW = 128
TOK_MOE = 128
TOPK = 2
FE = 768
SHARED = 512
EXPERTS = 16
CAP = 32
SEQ_ATT = 8192
TOKENS_MOE = 4096
N_EP = 8
N_TP = 4


def draw_att_queries(key, part):
    shape = (SEQ_ATT, KV_HEADS, HEADS // KV_HEADS, HEAD_DIM)
    base_draw = jax.random.truncated_normal(jax.random.fold_in(key, 21), -6.0, 6.0, shape, jnp.float32)
    return base_draw.reshape(SEQ_ATT, HEADS * HEAD_DIM).astype(jnp.bfloat16)


def draw_att_keys(key, part):
    shape = (SEQ_ATT, KV_HEADS, HEAD_DIM)
    base_draw = jax.random.truncated_normal(jax.random.fold_in(key, 31), -6.0, 6.0, shape, jnp.float32)
    return base_draw.reshape(SEQ_ATT, KV_HEADS * HEAD_DIM).astype(jnp.bfloat16)


def block_scale(stream_key, extent, cuts, least, largest):
    def one(dim, blocks):
        heights = jax.random.uniform(jax.random.fold_in(jax.random.fold_in(stream_key, 6), dim), (blocks,), jnp.float32, least / len(cuts), largest / len(cuts))
        return jnp.repeat(jnp.exp(heights), extent[dim] // blocks).reshape((-1,) + (1,) * (len(extent) - dim - 1))

    gain = one(*cuts[0])
    for cut in cuts[1:]:
        gain = gain * one(*cut)
    return gain


def deal_out(key, own, number, rows, amount, top, limit, lean):
    order = jax.random.permutation(key, amount)
    crowded, common = shares(amount, rows * top, limit, lean, True), shares(amount, rows * top, limit, lean, False)
    places = jnp.arange(amount)

    def named(tallies, rotation):
        used = int((tallies > 0).sum())
        fixed = max(1, used // 4)
        shifted = fixed + (places - fixed + rotation * (used - fixed)) % max(1, amount - fixed)
        return jnp.zeros((amount,), jnp.int32).at[order[jnp.where(places < fixed, places, shifted)]].set(jnp.asarray(tallies, jnp.int32))

    tallies = jnp.where(number % 4 == 0, named(crowded, number // 4), named(common, number - number // 4 - 1))
    mixed = jax.random.permutation(jax.random.fold_in(own, 3), amount)
    giver, taker = mixed[0:amount // 2 * 2:2], mixed[1:amount // 2 * 2:2]
    slack = jnp.minimum(tallies[giver] - 1, limit - tallies[taker]) // 2
    slack = jnp.where((giver == order[0]) | (taker == order[0]) | (tallies[taker] == 0), 0, jnp.maximum(slack, 0))
    shifted = jax.random.randint(jax.random.fold_in(own, 4), (amount // 2,), 0, 1 << 20) % (slack + 1)
    tallies = tallies.at[giver].add(-shifted).at[taker].add(shifted)
    members = jnp.searchsorted(jnp.cumsum(tallies), jnp.arange(rows * top), side="right").astype(jnp.int32)
    table = members.reshape(top, rows).T
    table = table[jax.random.permutation(jax.random.fold_in(own, 1), rows)]
    rotation = jax.random.randint(jax.random.fold_in(own, 2), (rows, 1), 0, top)
    return jnp.take_along_axis(table, (jnp.arange(top)[None, :] + rotation) % top, axis=1)


def shares(count, total, reach, lean, full):
    portions = [(1 << 20) // math.isqrt(rank ** lean) + 1 for rank in range(1, count + 1)]
    largest = reach if full else min(reach, max(-(-total // count), total * portions[0] // sum(portions)))
    least = 1 if total - largest >= count - 1 else 0
    given, rest = [largest] + [least] * (count - 1), total - largest - least * (count - 1)
    while rest > 0:
        free = [i for i in range(1, count) if given[i] < largest] or [i for i in range(1, count) if given[i] < reach]
        whole, budget = sum([portions[i] for i in free]), rest
        for i in free:
            more = min(reach - given[i], max(1, budget * portions[i] // whole), rest)
            given[i] = given[i] + more
            rest = rest - more
    return np.array(given)


def centred(stream_key, dims, width, reach, shards=(), kind=jnp.bfloat16):
    values = width * jax.random.normal(stream_key, dims, jnp.float32)
    if shards:
        values = values * block_scale(stream_key, dims, shards, -0.22, 0.18)
    return jnp.clip(values, -reach, reach).astype(kind)


def setup_inputs(seed: int = 0) -> dict:
    key_list = jax.random.split(jax.random.key(seed), 18)
    att_queries = draw_att_queries(jax.random.fold_in(key_list[17], 71), 0)
    att_keys = draw_att_keys(jax.random.fold_in(key_list[17], 71), 0)
    att_values = centred(key_list[2], (SEQ_ATT, KV_HEADS * HEAD_DIM), 1.0, 6.0, ((0, 32),))
    sink_logits = jnp.clip(jax.random.uniform(key_list[3], (HEADS,), jnp.float32, 3.0, 6.5), 3.0, 6.5)
    out_weight = centred(key_list[4], (HEADS * HEAD_DIM, D), (HEADS * HEAD_DIM) ** -0.5, 0.1875)
    att_gain = jnp.clip(1.0 + 0.18 * jax.random.normal(key_list[5], (D,), jnp.float32), 0.1, 1.9)
    moe_in = centred(key_list[6], (TOKENS_MOE, D), 1.0, 6.0, ((0, 32),))
    pre_gain = jnp.clip(1.0 + 0.18 * jax.random.normal(key_list[7], (D,), jnp.float32), 0.1, 1.9)
    expert_ids_keys = jax.random.split(jax.random.fold_in(key_list[8], 1), TOKENS_MOE // TOK_MOE)
    expert_ids_turns = jax.random.permutation(jax.random.fold_in(key_list[8], 3), TOKENS_MOE // TOK_MOE)
    expert_ids = jax.vmap(lambda own, number: deal_out(jax.random.fold_in(key_list[8], 2), own, number, TOK_MOE, EXPERTS, TOPK, CAP, 1))(expert_ids_keys, expert_ids_turns).reshape((TOKENS_MOE, TOPK))
    routed_expert_weight = jnp.clip(jnp.exp(math.log(1.5) - 2.014903 * jax.random.uniform(key_list[9], (TOKENS_MOE, TOPK), jnp.float32) ** block_scale(key_list[9], (TOKENS_MOE, TOPK), ((0, 32),), -0.2, 0.2)), 0.2, 1.5)
    w_gate = centred(key_list[10], (EXPERTS, D, FE), D ** -0.5, 0.125, ((0, 8), (2, 4)))
    w_up = centred(key_list[11], (EXPERTS, D, FE), D ** -0.5, 0.125, ((0, 8), (2, 4)))
    w_down = centred(key_list[12], (EXPERTS, FE, D), FE ** -0.5, 0.21875, ((0, 8), (1, 4)))
    common_expert_gate_weight = centred(key_list[13], (D, SHARED), D ** -0.5, 0.125, ((1, 4),))
    common_expert_up_weight = centred(key_list[14], (D, SHARED), D ** -0.5, 0.125, ((1, 4),))
    common_expert_down_weight = centred(key_list[15], (SHARED, D), SHARED ** -0.5, 0.25, ((0, 4),))
    moe_gain = jnp.clip(1.0 + 0.18 * jax.random.normal(key_list[16], (D,), jnp.float32), 0.1, 1.9)
    return {"att_queries": att_queries, "att_keys": att_keys, "att_values": att_values, "sink_logits": sink_logits, "out_weight": out_weight, "att_gain": att_gain, "moe_in": moe_in, "pre_gain": pre_gain, "expert_ids": expert_ids, "routed_expert_weight": routed_expert_weight, "w_gate": w_gate, "w_up": w_up, "w_down": w_down, "common_expert_gate_weight": common_expert_gate_weight, "common_expert_up_weight": common_expert_up_weight, "common_expert_down_weight": common_expert_down_weight, "moe_gain": moe_gain}


EPS = 1e-06
NEGATIVE = -1e+30

def rms_scale(inputs, gain_vec):
    mean_sq = lax.optimization_barrier(jnp.mean(inputs * inputs, axis=-1, keepdims=True))
    return inputs * lax.rsqrt(mean_sq + EPS) * gain_vec

def block_parts(hidden, down_rows, split_count):
    block_width = hidden.shape[-1] // split_count
    pieces = jnp.einsum('rbf,bfd->rbd', hidden.astype(jnp.float32).reshape(hidden.shape[0], split_count, block_width), down_rows.astype(jnp.float32).reshape(split_count, block_width, down_rows.shape[-1]))
    rounded = lax.optimization_barrier(pieces.astype(jnp.bfloat16))
    return lax.optimization_barrier(jnp.sum(rounded.astype(jnp.float32), axis=1))

def window_attention(att_queries, att_keys, att_values, sink_logits):
    group_size = HEADS // KV_HEADS
    blocks = SEQ_ATT // WINDOW
    padding = jnp.zeros((WINDOW, KV_HEADS * HEAD_DIM), att_keys.dtype)
    key_blocks = jnp.concatenate([padding, att_keys], axis=0).reshape(blocks + 1, WINDOW, KV_HEADS, HEAD_DIM)
    value_blocks = jnp.concatenate([padding, att_values], axis=0).reshape(blocks + 1, WINDOW, KV_HEADS, HEAD_DIM)
    query_blocks = att_queries.reshape(blocks, WINDOW, KV_HEADS, group_size, HEAD_DIM)
    distance = jnp.arange(WINDOW)[:, None] + WINDOW - jnp.arange(2 * WINDOW)[None, :]
    inside = (distance >= 0) & (distance < WINDOW)
    sink_grid = sink_logits.astype(jnp.float32).reshape(KV_HEADS, group_size)[:, :, None, None]
    score_scale = 1.0 / math.sqrt(HEAD_DIM)

    def one_block(block_index):
        key_band = lax.dynamic_slice_in_dim(key_blocks, block_index, 2, 0).reshape(2 * WINDOW, KV_HEADS, HEAD_DIM)
        value_band = lax.dynamic_slice_in_dim(value_blocks, block_index, 2, 0).reshape(2 * WINDOW, KV_HEADS, HEAD_DIM)
        query_block = lax.dynamic_index_in_dim(query_blocks, block_index, 0, keepdims=False)
        scores = jnp.einsum('qgjd,kgd->gjqk', query_block.astype(jnp.float32), key_band.astype(jnp.float32)) * score_scale
        key_pos = block_index * WINDOW - WINDOW + jnp.arange(2 * WINDOW)
        is_valid = inside & (key_pos >= 0)[None, :]
        scores = jnp.where(is_valid[None, None], scores, NEGATIVE)
        row_top = jnp.maximum(lax.optimization_barrier(jnp.max(scores, axis=-1, keepdims=True)), sink_grid)
        exp_scores = jnp.exp(scores - row_top)
        denominator = lax.optimization_barrier(jnp.sum(exp_scores, axis=-1, keepdims=True)) + jnp.exp(sink_grid - row_top)
        probs = (exp_scores / denominator).astype(jnp.bfloat16)
        head_mix = jnp.einsum('gjqk,kgd->qgjd', probs.astype(jnp.float32), value_band.astype(jnp.float32))
        return head_mix.astype(jnp.bfloat16).reshape(WINDOW, HEADS * HEAD_DIM)
    head_mix = lax.map(one_block, jnp.arange(blocks, dtype=jnp.int32))
    return head_mix.reshape(SEQ_ATT, HEADS * HEAD_DIM)

def routed_experts(normed, expert_ids, routed_expert_weight, w_gate, w_up, w_down):
    devices = N_EP * N_TP
    per_device = TOK_MOE * TOPK
    flat_ids = expert_ids.reshape(devices, per_device)
    earlier = jnp.arange(per_device)[None, :] < jnp.arange(per_device)[:, None]

    def positions_of(device_ids):
        return lax.optimization_barrier(jnp.sum((device_ids[:, None] == device_ids[None, :]) & earlier, axis=1)).astype(jnp.int32)
    position = lax.map(positions_of, flat_ids)
    device_index = jnp.arange(devices, dtype=jnp.int32)[:, None]
    slot_index = ((flat_ids * devices + device_index) * CAP + position).reshape(-1).astype(jnp.int32)
    token_index = (device_index * TOK_MOE + jnp.arange(per_device, dtype=jnp.int32)[None, :] // TOPK).reshape(-1)
    table_size = EXPERTS * devices * CAP
    row_table = jnp.zeros((table_size,), jnp.int32).at[slot_index].set(token_index.astype(jnp.int32))
    row_table = row_table.reshape(EXPERTS, devices * CAP)
    weight_table = jnp.zeros((table_size,), jnp.float32).at[slot_index].set(routed_expert_weight.reshape(-1))
    weight_table = weight_table.reshape(EXPERTS, devices * CAP)

    def add_expert(running, expert_index):
        row_ids = lax.dynamic_index_in_dim(row_table, expert_index, 0, keepdims=False)
        slot_weights = lax.dynamic_index_in_dim(weight_table, expert_index, 0, keepdims=False)
        picked = normed[row_ids]
        gate_act = jnp.dot(picked, w_gate[expert_index], preferred_element_type=jnp.float32)
        up_act = jnp.dot(picked, w_up[expert_index], preferred_element_type=jnp.float32)
        hidden = (jax.nn.silu(gate_act) * up_act).astype(jnp.bfloat16)
        output = block_parts(hidden, w_down[expert_index], N_TP).astype(jnp.bfloat16)
        running = running.at[row_ids].add(slot_weights[:, None] * output.astype(jnp.float32))
        return (running, None)
    start_value = jnp.zeros((TOKENS_MOE, D), jnp.float32)
    return lax.scan(add_expert, start_value, jnp.arange(EXPERTS, dtype=jnp.int32))[0]

def reference(att_queries, att_keys, att_values, sink_logits, out_weight, att_gain, moe_in, pre_gain, expert_ids, routed_expert_weight, w_gate, w_up, w_down, common_expert_gate_weight, common_expert_up_weight, common_expert_down_weight, moe_gain):
    head_mix = window_attention(att_queries, att_keys, att_values, sink_logits)
    projected = jnp.dot(head_mix, out_weight, preferred_element_type=jnp.float32)
    mixer_out = rms_scale(projected, att_gain).astype(jnp.bfloat16)
    normed = rms_scale(moe_in.astype(jnp.float32), pre_gain).astype(jnp.bfloat16)
    routed = routed_experts(normed, expert_ids, routed_expert_weight, w_gate, w_up, w_down)

    def shared_rows(row_block):
        gate_act = jnp.dot(row_block, common_expert_gate_weight, preferred_element_type=jnp.float32)
        up_act = jnp.dot(row_block, common_expert_up_weight, preferred_element_type=jnp.float32)
        common_expert_hidden = (jax.nn.silu(gate_act) * up_act).astype(jnp.bfloat16)
        return block_parts(common_expert_hidden, common_expert_down_weight, N_TP)
    shared_sum = lax.map(shared_rows, normed.reshape(N_EP * N_TP, TOK_MOE, D)).reshape(TOKENS_MOE, D)
    combined = routed + shared_sum
    experts_out = rms_scale(combined, moe_gain).astype(jnp.bfloat16)
    return (mixer_out, experts_out)
```

```python
import functools
import math

import jax
import jax.numpy as jnp
from jax import lax
from jax.experimental import pallas as pl
from jax.experimental.pallas import tpu as pltpu
from jax.sharding import PartitionSpec as P

HEADS = 16
KV_HEADS = 4
HEAD_DIM = 64
WINDOW = 128

EPS = 1e-06
NEGATIVE = -1e30
PLANES = 2
CHUNKS = 4
ROW_TILE = 8

VMEM = pl.BlockSpec(memory_space=pltpu.VMEM)
SMEM = pl.BlockSpec(memory_space=pltpu.SMEM)
ANY = pl.BlockSpec(memory_space=pl.ANY)
F32 = jnp.float32
BF16 = jnp.bfloat16
MESH = pl.DeviceIdType.MESH
NT = (((1,), (1,)), ((), ()))
TN = (((0,), (0,)), ((), ()))


def iota(shape, dim):
    return lax.broadcasted_iota(jnp.int32, shape, dim)


def rms_scale(inputs, gain_vec):
    mean_sq = jnp.mean(inputs * inputs, axis=-1, keepdims=True)
    return inputs * lax.rsqrt(mean_sq + EPS) * gain_vec


def silu(v):
    return v / (1.0 + jnp.exp(-v))


def flip(index, amount):
    bit = 1
    while bit <= amount:
        if amount & bit:
            index = index + bit - 2 * bit * lax.rem(index // bit, 2)
        bit *= 2
    return index


class Sems:
    def __init__(self, *arrays):
        self.arrays, self.used = arrays, 0

    def take(self):
        self.used += 1
        return [array.at[self.used - 1] for array in self.arrays]


def layer_kernel(
    n_ep,
    n_tp,
    cap,
    sink_ref,
    ids_ref,
    weight_ref,
    pre_gain_ref,
    att_gain_ref,
    moe_gain_ref,
    q_hbm,
    k_hbm,
    v_hbm,
    out_w_hbm,
    x_hbm,
    gate_hbm,
    up_hbm,
    down_hbm,
    common_gate_hbm,
    common_up_hbm,
    common_down_hbm,
    mixer_hbm,
    experts_ref,
    x_v,
    normed,
    far_normed,
    far_ids,
    far_weight,
    chosen,
    packed,
    arrived,
    outs,
    returned,
    gate_v,
    up_v,
    down_v,
    act,
    hidden,
    common_gate,
    common_up,
    common_down,
    shared,
    part_out,
    part_in,
    q_v,
    k_v,
    v_v,
    rim_k,
    rim_v,
    out_w,
    mix,
    mixer,
    local_sems,
    send_sems,
    recv_sems,
    row_send,
    row_recv,
    ack_sem,
):
    far = n_tp // PLANES
    tokens, d = x_v.shape
    top = ids_ref.shape[0]
    slots = n_ep * cap
    width = gate_hbm.shape[1]
    half = far * width
    cw = d // CHUNKS
    me_e, me_t = lax.axis_index("ep"), lax.axis_index("tp")
    plane = me_t // far
    away = flip(me_t, far)
    mates = [flip(me_t, j) for j in range(1, far)]
    devices = n_ep * n_tp
    me = me_e * n_tp + me_t
    after, before = lax.rem(me + 1, devices), lax.rem(me + devices - 1, devices)
    local, net = Sems(local_sems), Sems(send_sems, recv_sems)
    sent = []

    def fetch(src, dst):
        copy = pltpu.make_async_copy(src, dst, local.take()[0])
        copy.start()
        return copy

    def remote(src, dst, e, t, start=True):
        send, recv = net.take()
        copy = pltpu.make_async_remote_copy(
            src, dst, send, recv, device_id=(e, t), device_id_type=MESH
        )
        if start:
            copy.start()
        sent.append(copy)
        return copy

    def rows_of(group):
        return pl.ds(pl.multiple_of(group * cap, cap), cap)

    def exchange(phase, src, dst, act_on):
        def step(j, carry):
            to = lax.rem(me_e + j, n_ep)
            copy = pltpu.make_async_remote_copy(
                src.at[rows_of(to)],
                dst.at[rows_of(me_e)],
                row_send.at[phase, j],
                row_recv.at[phase, j],
                device_id=(to, me_t),
                device_id_type=MESH,
            )
            act_on(copy)
            return carry

        lax.fori_loop(1, n_ep, step, 0)

    def start_rows(phase, src, dst):
        exchange(phase, src, dst, lambda copy: copy.start())
        dst[rows_of(me_e), :] = src[rows_of(me_e), :]

    def wait_rows(phase, src, dst):
        exchange(phase, src, dst, lambda copy: copy.wait_recv())

    load_x = fetch(x_hbm, x_v)
    barrier = pltpu.get_barrier_semaphore()

    def greet(j, carry):
        pl.semaphore_signal(
            barrier, inc=1, device_id=(lax.rem(me_e + j, n_ep), me_t), device_id_type=MESH
        )
        return carry

    lax.fori_loop(1, n_ep, greet, 0)
    for t in [away] + mates:
        pl.semaphore_signal(barrier, inc=1, device_id=(me_e, t), device_id_type=MESH)
    for n in (after, before):
        pl.semaphore_signal(
            barrier, inc=1, device_id=(n // n_tp, lax.rem(n, n_tp)), device_id_type=MESH
        )
    own_loads = []
    for src, dst in ((gate_hbm, gate_v), (up_hbm, up_v), (down_hbm, down_v)):
        own_loads.append(fetch(src.at[plane], dst.at[0]))
    load_q = [fetch(q_hbm, q_v), fetch(k_hbm, k_v), fetch(v_hbm, v_v), fetch(out_w_hbm, out_w)]
    common_cols = common_gate_hbm.shape[1]
    common_loads = [
        fetch(common_gate_hbm, common_gate.at[:, pl.ds(0, common_cols)]),
        fetch(common_up_hbm, common_up.at[:, pl.ds(0, common_cols)]),
        fetch(common_down_hbm, common_down.at[pl.ds(0, common_cols)]),
    ]
    pl.semaphore_wait(barrier, n_ep - 1 + far + 2)

    cut = width // 4
    first_rows, last_rows = pl.ds(0, cut), pl.ds(cut, width - cut)
    other = PLANES - 1 - plane
    gate_far = [
        remote(gate_hbm.at[other, first_rows], gate_v.at[far, first_rows], me_e, away),
    ]
    meta = [
        remote(ids_ref, far_ids, me_e, away),
        remote(weight_ref, far_weight, me_e, away),
    ]
    mate_common, mate_kept = [], []
    for j, t in enumerate(mates, 1):
        cols = pl.ds(j * common_cols, common_cols)
        mate_common.append(remote(common_gate_hbm, common_gate.at[:, cols], me_e, t))
        mate_common.append(remote(common_up_hbm, common_up.at[:, cols], me_e, t))
        mate_common.append(remote(common_down_hbm, common_down.at[cols], me_e, t))
    edge = k_hbm.shape[0] - WINDOW
    after_at = (after // n_tp, lax.rem(after, n_tp))
    rims = [
        remote(k_hbm.at[pl.ds(edge, WINDOW)], rim_k, *after_at),
        remote(v_hbm.at[pl.ds(edge, WINDOW)], rim_v, *after_at),
    ]

    load_x.wait()
    normed[...] = rms_scale(x_v[...].astype(F32), pre_gain_ref[...]).astype(BF16)
    normed_far = remote(normed, far_normed, me_e, away)
    gate_far.append(remote(gate_hbm.at[other, last_rows], gate_v.at[far, last_rows], me_e, away))
    up_halves = [pl.ds(0, width // 2), pl.ds(width // 2, width // 2)]
    up_far = [
        remote(up_hbm.at[other, rows], up_v.at[far, rows], me_e, away) for rows in up_halves
    ]
    chunks = [pl.ds(c * cw, cw) for c in range(CHUNKS)]
    down_far = [
        remote(down_hbm.at[other, :, cols], down_v.at[far, :, cols], me_e, away)
        for cols in chunks
    ]

    earlier = (iota((tokens, tokens), 0) < iota((tokens, tokens), 1)).astype(F32).astype(BF16)

    def route(ids, side):
        numbers = iota((n_ep, tokens), 0) * PLANES + plane
        hits = [numbers == ids[k : k + 1, :] for k in range(top)]
        hit = functools.reduce(lambda a, b: a | b, hits).astype(F32).astype(BF16)
        count = jnp.dot(hit, earlier, preferred_element_type=F32)
        place = count + (iota((n_ep, tokens), 0) * cap + 1).astype(F32)
        slot_number = (iota((slots, tokens), 0) + 1).astype(F32)
        total = None
        for k in range(top):
            slot = jnp.sum(jnp.where(hits[k], place, 0.0), axis=0, keepdims=True)
            one_hot = (slot_number == slot).astype(F32).astype(BF16)
            chosen[side, :, k * tokens : (k + 1) * tokens] = one_hot
            total = one_hot if total is None else total + one_hot
        return total

    def pack(ids, side, rows_ref):
        one_hot = route(ids, side)
        rows = rows_ref[...]
        step = slots // 2
        for i in range(2):
            packed[side, i * step : (i + 1) * step, :] = jnp.dot(
                one_hot[i * step : (i + 1) * step], rows, preferred_element_type=F32
            ).astype(BF16)
        start_rows(side, packed.at[side], arrived.at[side])

    pack(ids_ref[...], 0, normed)
    for j, t in enumerate(mates, 1):
        for src, dst in ((gate_hbm, gate_v), (up_hbm, up_v), (down_hbm, down_v)):
            mate_kept.append(remote(src.at[plane], dst.at[j], me_e, t))

    group_size = HEADS // KV_HEADS
    blocks = q_v.shape[0] // WINDOW
    shape = (WINDOW, 2 * WINDOW)
    gap = iota(shape, 0) + WINDOW - iota(shape, 1)
    inside = (gap >= 0) & (gap < WINDOW)

    def attend(n):
        rows = pl.ds(n * WINDOW, WINDOW)
        valid = inside
        if n == 0:
            valid = inside & (iota(shape, 1) + me * q_v.shape[0] >= WINDOW)
        for g in range(KV_HEADS):
            cols = pl.ds(g * HEAD_DIM, HEAD_DIM)
            if n == 0:
                keys = jnp.concatenate([rim_k[:, cols], k_v[rows, cols]], axis=0)
                values = jnp.concatenate([rim_v[:, cols], v_v[rows, cols]], axis=0)
            else:
                band = pl.ds((n - 1) * WINDOW, 2 * WINDOW)
                keys, values = k_v[band, cols], v_v[band, cols]
            mixed = []
            for j in range(group_size):
                h = g * group_size + j
                query = q_v[rows, pl.ds(h * HEAD_DIM, HEAD_DIM)]
                scores = lax.dot_general(query, keys, NT, preferred_element_type=F32) * (
                    1.0 / math.sqrt(HEAD_DIM)
                )
                scores = jnp.where(valid, scores, NEGATIVE)
                sink = sink_ref[h]
                row_top = jnp.maximum(jnp.max(scores, axis=-1, keepdims=True), sink)
                weights = jnp.exp(scores - row_top)
                total = jnp.sum(weights, axis=-1, keepdims=True) + jnp.exp(sink - row_top)
                probs = (weights * (1.0 / total)).astype(BF16)
                mixed.append(jnp.dot(probs, values, preferred_element_type=F32).astype(BF16))
            span = group_size * HEAD_DIM
            mix[rows, pl.ds(g * span, span)] = jnp.concatenate(mixed, axis=1)

    def project(n):
        rows = pl.ds(n * WINDOW, WINDOW)
        projected = jnp.dot(mix[rows, :], out_w[...], preferred_element_type=F32)
        mixer[rows, :] = rms_scale(projected, att_gain_ref[...]).astype(BF16)
        return fetch(mixer.at[rows], mixer_hbm.at[rows])

    def relay(copy, view):
        copy.wait_recv()
        return [remote(view(far), view(far + j), me_e, t) for j, t in enumerate(mates, 1)]

    for load in load_q[:3]:
        load.wait()
    for n in range(1, blocks):
        attend(n)
    gate_mate = relay(gate_far[0], lambda b: gate_v.at[b, first_rows])
    for copy in rims:
        copy.wait_recv()
    before_at = (before // n_tp, lax.rem(before, n_tp))
    pl.semaphore_signal(ack_sem, inc=1, device_id=before_at, device_id_type=MESH)
    attend(0)
    load_q[3].wait()
    mixer_copies = [project(n) for n in range(blocks)]

    def share(side, rows_ref):
        rows = rows_ref[...]
        gate = jnp.dot(rows, common_gate[...], preferred_element_type=F32)
        up = jnp.dot(rows, common_up[...], preferred_element_type=F32)
        units = (silu(gate) * up).astype(BF16)
        shared[side] = jnp.dot(units, common_down[...], preferred_element_type=F32)

    for load in common_loads:
        load.wait()
    for copy in mate_common:
        copy.wait_recv()
    share(0, normed)

    for copy in meta:
        copy.wait_recv()
    normed_far.wait_recv()
    pack(far_ids[...], 1, far_normed)
    share(1, far_normed)

    def product(side, weights, low, count):
        rows = arrived[side]
        matrix = weights[low : low + count].reshape(count * width, d)
        return lax.dot_general(rows, matrix, NT, preferred_element_type=F32)

    gate_mate += relay(gate_far[1], lambda b: gate_v.at[b, last_rows])
    for load in own_loads:
        load.wait()
    for copy in mate_kept:
        copy.wait_recv()
    for copy in gate_mate:
        copy.wait_recv()
    wait_rows(0, packed.at[0], arrived.at[0])
    act[0] = silu(product(0, gate_v, 0, 2 * far))
    hidden[0, :, :half] = (act[0, :, :half] * product(0, up_v, 0, far)).astype(BF16)
    up_mate = relay(up_far[0], lambda b: up_v.at[b, up_halves[0]])
    wait_rows(1, packed.at[1], arrived.at[1])
    act[1] = silu(product(1, gate_v, 0, 2 * far))
    hidden[1, :, :half] = (act[1, :, :half] * product(1, up_v, 0, far)).astype(BF16)
    up_mate += relay(up_far[1], lambda b: up_v.at[b, up_halves[1]])
    for copy in up_mate:
        copy.wait_recv()
    for side in range(2):
        hidden[side, :, half:] = (act[side, :, half:] * product(side, up_v, far, far)).astype(BF16)

    def phase(side, c):
        return 2 + side * CHUNKS + c

    down_mate = []
    for c, cols in enumerate(chunks):
        for copy in relay(down_far[c], lambda b, cols=cols: down_v.at[b, :, cols]):
            copy.wait_recv()
        matrix = down_v[:, :, cols].reshape(2 * half, cw)
        for side in (1, 0) if c else (0, 1):
            outs[side, c] = jnp.dot(hidden[side], matrix, preferred_element_type=F32).astype(BF16)
            start_rows(phase(side, c), outs.at[side, c], returned.at[side, c])

    eye = iota((tokens, tokens), 0) == iota((tokens, tokens), 1)

    def columns_of(weights):
        return [
            jnp.sum(jnp.where(eye, weights[k : k + 1, :], 0.0), axis=1, keepdims=True)
            for k in range(top)
        ]

    scales = [columns_of(weight_ref[...]), columns_of(far_weight[...])]

    def combine(side, c):
        wait_rows(phase(side, c), outs.at[side, c], returned.at[side, c])
        picked = lax.dot_general(
            chosen[side], returned[side, c], TN, preferred_element_type=F32
        )
        total = shared[side, :, chunks[c]]
        for k in range(top):
            total = total + scales[side][k] * picked[k * tokens : (k + 1) * tokens]
        return total

    parts = []
    for c, cols in enumerate(chunks):
        for side in (1, 0) if c else (0, 1):
            if side:
                part_out[c] = combine(1, c).astype(BF16)
                parts.append(remote(part_out.at[c], part_in.at[c], me_e, away))
            else:
                shared[0, :, cols] = combine(0, c)
    square = jnp.zeros((tokens, 1), F32)
    for c, cols in enumerate(chunks):
        parts[c].wait_recv()
        total = shared[0, :, cols] + part_in[c].astype(F32)
        shared[0, :, cols] = total
        square = square + jnp.sum(total * total, axis=-1, keepdims=True)
    scale = lax.rsqrt(square * (1.0 / d) + EPS)
    experts_ref[...] = (shared[0] * scale * moe_gain_ref[...]).astype(BF16)

    for copy in mixer_copies:
        copy.wait()
    for copy in sent:
        copy.wait_send()
    for side in range(2):
        exchange(side, packed.at[side], arrived.at[side], lambda copy: copy.wait_send())
        for c in range(CHUNKS):
            exchange(
                phase(side, c),
                outs.at[side, c],
                returned.at[side, c],
                lambda copy: copy.wait_send(),
            )
    pl.semaphore_wait(ack_sem, 1)


def body(
    att_queries,
    att_keys,
    att_values,
    sink_logits,
    out_weight,
    att_gain,
    moe_in,
    pre_gain,
    expert_ids,
    routed_expert_weight,
    w_gate,
    w_up,
    w_down,
    common_expert_gate_weight,
    common_expert_up_weight,
    common_expert_down_weight,
    moe_gain,
):
    assert w_gate.shape[0] == PLANES
    n_ep, n_tp = lax.axis_size("ep"), lax.axis_size("tp")
    rows, width = att_queries.shape
    tokens, d = moe_in.shape
    top = expert_ids.shape[1]
    slot_cap = 2 * tokens * top // (PLANES * n_ep)
    cap = -(-slot_cap // ROW_TILE) * ROW_TILE
    slots = cap * n_ep
    far = n_tp // PLANES
    blocks = 2 * far
    kv = att_keys.shape[1]
    units = w_gate.shape[2]
    common = common_expert_gate_weight.shape[1]
    cw = d // CHUNKS
    scratch = [
        pltpu.VMEM((tokens, d), BF16),
        pltpu.VMEM((tokens, d), BF16),
        pltpu.VMEM((tokens, d), BF16),
        pltpu.VMEM((top, tokens), jnp.int32),
        pltpu.VMEM((top, tokens), F32),
        pltpu.VMEM((2, slots, top * tokens), BF16),
        pltpu.VMEM((2, slots, d), BF16),
        pltpu.VMEM((2, slots, d), BF16),
        pltpu.VMEM((2, CHUNKS, slots, cw), BF16),
        pltpu.VMEM((2, CHUNKS, slots, cw), BF16),
        pltpu.VMEM((blocks, units, d), BF16),
        pltpu.VMEM((blocks, units, d), BF16),
        pltpu.VMEM((blocks, units, d), BF16),
        pltpu.VMEM((2, slots, blocks * units), F32),
        pltpu.VMEM((2, slots, blocks * units), BF16),
        pltpu.VMEM((d, far * common), BF16),
        pltpu.VMEM((d, far * common), BF16),
        pltpu.VMEM((far * common, d), BF16),
        pltpu.VMEM((2, tokens, d), F32),
        pltpu.VMEM((CHUNKS, tokens, cw), BF16),
        pltpu.VMEM((CHUNKS, tokens, cw), BF16),
        pltpu.VMEM((rows, width), BF16),
        pltpu.VMEM((rows, kv), BF16),
        pltpu.VMEM((rows, kv), BF16),
        pltpu.VMEM((WINDOW, kv), BF16),
        pltpu.VMEM((WINDOW, kv), BF16),
        pltpu.VMEM(out_weight.shape, BF16),
        pltpu.VMEM((rows, width), BF16),
        pltpu.VMEM((rows, d), BF16),
        pltpu.SemaphoreType.DMA((11 + rows // WINDOW,)),
        pltpu.SemaphoreType.DMA((9 + 2 * CHUNKS + (far - 1) * (10 + CHUNKS),)),
        pltpu.SemaphoreType.DMA((9 + 2 * CHUNKS + (far - 1) * (10 + CHUNKS),)),
        pltpu.SemaphoreType.DMA((2 + 2 * CHUNKS, n_ep)),
        pltpu.SemaphoreType.DMA((2 + 2 * CHUNKS, n_ep)),
        pltpu.SemaphoreType.REGULAR,
    ]
    return pl.pallas_call(
        functools.partial(layer_kernel, n_ep, n_tp, cap),
        out_shape=(
            jax.ShapeDtypeStruct((rows, d), BF16),
            jax.ShapeDtypeStruct((tokens, d), BF16),
        ),
        in_specs=[SMEM] + [VMEM] * 5 + [ANY] * 11,
        out_specs=(ANY, VMEM),
        scratch_shapes=scratch,
        compiler_params=pltpu.CompilerParams(
            vmem_limit_bytes=63 * 1024 * 1024, collective_id=0, has_side_effects=True
        ),
        name="layer",
    )(
        sink_logits,
        expert_ids.T,
        routed_expert_weight.T,
        pre_gain[None],
        att_gain[None],
        moe_gain[None],
        att_queries,
        att_keys,
        att_values,
        out_weight,
        moe_in,
        jnp.swapaxes(w_gate, 1, 2),
        jnp.swapaxes(w_up, 1, 2),
        w_down,
        common_expert_gate_weight,
        common_expert_up_weight,
        common_expert_down_weight,
    )


def solution(mesh):
    tokens_spec = P(("ep", "tp"), None)
    in_specs = (
        tokens_spec,
        tokens_spec,
        tokens_spec,
        P(),
        P(),
        P(),
        tokens_spec,
        P(),
        tokens_spec,
        tokens_spec,
        P("ep", None, "tp"),
        P("ep", None, "tp"),
        P("ep", "tp", None),
        P(None, "tp"),
        P(None, "tp"),
        P("tp", None),
        P(),
    )
    return jax.shard_map(
        body, mesh=mesh, in_specs=in_specs, out_specs=(tokens_spec, tokens_spec), check_vma=False
    )
```

```python
import functools
import math

import jax
import jax.numpy as jnp
from jax import lax
from jax.experimental import pallas as pl
from jax.experimental.pallas import tpu as pltpu
from jax.sharding import PartitionSpec as P

HEADS = 16
KV_HEADS = 4
HEAD_DIM = 64
WINDOW = 128

EPS = 1e-06
NEGATIVE = -1e30
PLANES = 2
CHUNKS = 4
AHEAD = 2
EARLY = 2
ROW_TILE = 8
PAIR = 2
LINE = 4

VMEM = pl.BlockSpec(memory_space=pltpu.VMEM)
SMEM = pl.BlockSpec(memory_space=pltpu.SMEM)
ANY = pl.BlockSpec(memory_space=pl.ANY)
F32 = jnp.float32
BF16 = jnp.bfloat16
MESH = pl.DeviceIdType.MESH
NT = (((1,), (1,)), ((), ()))
TN = (((0,), (0,)), ((), ()))


def iota(shape, dim):
    return lax.broadcasted_iota(jnp.int32, shape, dim)


def rms_scale(inputs, gain_vec):
    mean_sq = jnp.mean(inputs * inputs, axis=-1, keepdims=True)
    return inputs * lax.rsqrt(mean_sq + EPS) * gain_vec


def silu(v):
    return v / (1.0 + jnp.exp(-v))


def flip(index, amount):
    bit = 1
    while bit <= amount:
        if amount & bit:
            index = index + bit - 2 * bit * lax.rem(index // bit, 2)
        bit *= 2
    return index


class Sems:
    def __init__(self, *arrays):
        self.arrays, self.used = arrays, 0

    def take(self):
        self.used += 1
        return [array.at[self.used - 1] for array in self.arrays]


def layer_kernel(
    n_ep,
    n_tp,
    cap,
    sink_ref,
    ids_ref,
    weight_ref,
    pre_gain_ref,
    att_gain_ref,
    moe_gain_ref,
    q_hbm,
    k_hbm,
    v_hbm,
    out_w_hbm,
    x_hbm,
    gate_hbm,
    up_hbm,
    down_hbm,
    common_gate_hbm,
    common_up_hbm,
    common_down_hbm,
    mixer_ref,
    experts_ref,
    x_v,
    normed,
    far_normed,
    far_ids,
    far_weight,
    chosen,
    packed,
    arrived,
    outs,
    returned,
    gate_v,
    up_v,
    down_v,
    act,
    hidden,
    common_gate,
    common_up,
    common_down,
    shared,
    part_out,
    part_in,
    q_v,
    k_v,
    v_v,
    rim_k,
    rim_v,
    out_w,
    mix,
    local_sems,
    send_sems,
    recv_sems,
    row_send,
    row_recv,
    ack_sem,
    *merge_refs,
):
    far = n_tp // PLANES
    tokens, d = x_v.shape
    top = ids_ref.shape[0]
    merging = bool(merge_refs)
    if merging:
        (
            home_ids,
            home_weight,
            home_chosen,
            home_rows,
            home_sums,
            home_out,
            home_in,
            meta_send,
            meta_recv,
            home_send,
            home_recv,
        ) = merge_refs
    slots = n_ep * cap
    width = gate_hbm.shape[1]
    half = far * width
    cw = d // CHUNKS
    me_e, me_t = lax.axis_index("ep"), lax.axis_index("tp")
    plane = me_t // far
    away = flip(me_t, far)
    mates = [flip(me_t, j) for j in range(1, far)]
    devices = n_ep * n_tp
    me = me_e * n_tp + me_t
    after, before = lax.rem(me + 1, devices), lax.rem(me + devices - 1, devices)
    local, net = Sems(local_sems), Sems(send_sems, recv_sems)

    line, spot = me_e // PAIR, lax.rem(me_e, PAIR)
    last = LINE - 1
    upper = line // (LINE // 2)
    home_line = last * (1 - upper)
    at_end = lax.rem(line, last) == 0
    end_flag = 1 - (lax.rem(line, last) + 1) // 2
    pair_e = line * PAIR + 1 - spot
    sent = []

    def fetch(src, dst):
        copy = pltpu.make_async_copy(src, dst, local.take()[0])
        copy.start()
        return copy

    def remote(src, dst, e, t, start=True):
        send, recv = net.take()
        copy = pltpu.make_async_remote_copy(
            src, dst, send, recv, device_id=(e, t), device_id_type=MESH
        )
        if start:
            copy.start()
        sent.append(copy)
        return copy

    def rows_of(group):
        return pl.ds(pl.multiple_of(group * cap, cap), cap)

    def exchange(phase, src, dst, act_on, wanted=None, first=1, stride=1):
        def step(i, carry):
            j = first + stride * i
            to = lax.rem(me_e + j, n_ep)
            copy = pltpu.make_async_remote_copy(
                src.at[rows_of(to)],
                dst.at[rows_of(me_e)],
                row_send.at[phase, j],
                row_recv.at[phase, j],
                device_id=(to, me_t),
                device_id_type=MESH,
            )
            if wanted is None:
                act_on(copy)
            else:
                pl.when(wanted(j))(lambda: act_on(copy))
            return carry

        lax.fori_loop(0, (n_ep - first + stride - 1) // stride, step, 0)

    def is_sent(j):
        return lax.rem(me_e + j, n_ep) // PAIR != home_line

    def is_received(j):
        source = lax.rem(me_e + n_ep - j, n_ep) // PAIR
        return line != last * (1 - source // (LINE // 2))

    def keep_rows(src, dst):
        dst[rows_of(me_e), :] = src[rows_of(me_e), :]

    def wait_rows(phase, src, dst, back=False):
        wanted = is_received if back and merging else None
        exchange(phase, src, dst, lambda copy: copy.wait_recv(), wanted)

    load_x = fetch(x_hbm, x_v)
    barrier = pltpu.get_barrier_semaphore()

    def greet(j, carry):
        pl.semaphore_signal(
            barrier, inc=1, device_id=(lax.rem(me_e + j, n_ep), me_t), device_id_type=MESH
        )
        return carry

    lax.fori_loop(1, n_ep, greet, 0)
    for t in [away] + mates:
        pl.semaphore_signal(barrier, inc=1, device_id=(me_e, t), device_id_type=MESH)
    for n in (after, before):
        pl.semaphore_signal(
            barrier, inc=1, device_id=(n // n_tp, lax.rem(n, n_tp)), device_id_type=MESH
        )
    if merging:
        pl.semaphore_signal(barrier, inc=1, device_id=(pair_e, away), device_id_type=MESH)
    own_loads = []
    for src, dst in ((gate_hbm, gate_v), (up_hbm, up_v), (down_hbm, down_v)):
        own_loads.append(fetch(src.at[plane], dst.at[0]))
    load_q = [fetch(q_hbm, q_v), fetch(k_hbm, k_v), fetch(v_hbm, v_v), fetch(out_w_hbm, out_w)]
    common_cols = common_gate_hbm.shape[1]
    common_loads = [
        fetch(common_gate_hbm, common_gate.at[:, pl.ds(0, common_cols)]),
        fetch(common_up_hbm, common_up.at[:, pl.ds(0, common_cols)]),
        fetch(common_down_hbm, common_down.at[pl.ds(0, common_cols)]),
    ]
    pl.semaphore_wait(barrier, n_ep - 1 + far + 2 + int(merging))

    cut = width // 4
    first_rows, last_rows = pl.ds(0, cut), pl.ds(cut, width - cut)
    other = PLANES - 1 - plane
    gate_far = [
        remote(gate_hbm.at[other, first_rows], gate_v.at[far, first_rows], me_e, away),
    ]
    meta = [
        remote(ids_ref, far_ids, me_e, away),
        remote(weight_ref, far_weight, me_e, away),
    ]
    mate_common, mate_kept = [], []
    for j, t in enumerate(mates, 1):
        cols = pl.ds(j * common_cols, common_cols)
        mate_common.append(remote(common_gate_hbm, common_gate.at[:, cols], me_e, t))
        mate_common.append(remote(common_up_hbm, common_up.at[:, cols], me_e, t))
        mate_common.append(remote(common_down_hbm, common_down.at[cols], me_e, t))
    edge = k_hbm.shape[0] - WINDOW
    after_at = (after // n_tp, lax.rem(after, n_tp))
    rims = [
        remote(k_hbm.at[pl.ds(edge, WINDOW)], rim_k, *after_at),
        remote(v_hbm.at[pl.ds(edge, WINDOW)], rim_v, *after_at),
    ]

    def home_meta(n):
        lines = (LINE // 2 - upper, last - line)
        to = lines[n] * PAIR + spot
        return [
            pltpu.make_async_remote_copy(
                src,
                dst,
                meta_send.at[n, i],
                meta_recv.at[i],
                device_id=(to, me_t),
                device_id_type=MESH,
            )
            for i, (src, dst) in enumerate(((ids_ref, home_ids), (weight_ref, home_weight)))
        ]

    if merging:

        @pl.when(at_end)
        def _():
            for n in range(2):
                for copy in home_meta(n):
                    copy.start()

    load_x.wait()
    normed[...] = rms_scale(x_v[...].astype(F32), pre_gain_ref[...]).astype(BF16)
    normed_far = remote(normed, far_normed, me_e, away)
    gate_far.append(remote(gate_hbm.at[other, last_rows], gate_v.at[far, last_rows], me_e, away))
    up_halves = [pl.ds(0, width // 2), pl.ds(width // 2, width // 2)]
    up_far = [
        remote(up_hbm.at[other, rows], up_v.at[far, rows], me_e, away) for rows in up_halves
    ]
    chunks = [pl.ds(c * cw, cw) for c in range(CHUNKS)]
    down_far = [
        remote(down_hbm.at[other, :, cols], down_v.at[far, :, cols], me_e, away, c < AHEAD)
        for c, cols in enumerate(chunks)
    ]

    earlier = (iota((tokens, tokens), 0) < iota((tokens, tokens), 1)).astype(F32).astype(BF16)

    def route(ids, numbers, chosen_ref):
        hits = [numbers == ids[k : k + 1, :] for k in range(top)]
        hit = functools.reduce(lambda a, b: a | b, hits).astype(F32).astype(BF16)
        count = jnp.dot(hit, earlier, preferred_element_type=F32)
        place = count + (iota(numbers.shape, 0) * cap + 1).astype(F32)
        slot_number = (iota((chosen_ref.shape[0], tokens), 0) + 1).astype(F32)
        total = None
        for k in range(top):
            slot = jnp.sum(jnp.where(hits[k], place, 0.0), axis=0, keepdims=True)
            one_hot = (slot_number == slot).astype(F32).astype(BF16)
            chosen_ref[:, k * tokens : (k + 1) * tokens] = one_hot
            total = one_hot if total is None else total + one_hot
        return total

    def pack(ids, side, rows_ref):
        numbers = iota((n_ep, tokens), 0) * PLANES + plane
        one_hot = route(ids, numbers, chosen.at[side])
        rows = rows_ref[...]
        step = slots // 2
        for i in range(2):
            packed[side, i * step : (i + 1) * step, :] = jnp.dot(
                one_hot[i * step : (i + 1) * step], rows, preferred_element_type=F32
            ).astype(BF16)
        exchange(side, packed.at[side], arrived.at[side], lambda copy: copy.start())
        keep_rows(packed.at[side], arrived.at[side])

    pack(ids_ref[...], 0, normed)
    for j, t in enumerate(mates, 1):
        for src, dst in ((gate_hbm, gate_v), (up_hbm, up_v), (down_hbm, down_v)):
            mate_kept.append(remote(src.at[plane], dst.at[j], me_e, t))

    group_size = HEADS // KV_HEADS
    blocks = q_v.shape[0] // WINDOW
    shape = (WINDOW, 2 * WINDOW)
    gap = iota(shape, 0) + WINDOW - iota(shape, 1)
    inside = (gap >= 0) & (gap < WINDOW)

    def attend(n):
        rows = pl.ds(n * WINDOW, WINDOW)
        valid = inside
        if n == 0:
            valid = inside & (iota(shape, 1) + me * q_v.shape[0] >= WINDOW)
        for g in range(KV_HEADS):
            cols = pl.ds(g * HEAD_DIM, HEAD_DIM)
            if n == 0:
                keys = jnp.concatenate([rim_k[:, cols], k_v[rows, cols]], axis=0)
                values = jnp.concatenate([rim_v[:, cols], v_v[rows, cols]], axis=0)
            else:
                band = pl.ds((n - 1) * WINDOW, 2 * WINDOW)
                keys, values = k_v[band, cols], v_v[band, cols]
            mixed = []
            for j in range(group_size):
                h = g * group_size + j
                query = q_v[rows, pl.ds(h * HEAD_DIM, HEAD_DIM)]
                scores = lax.dot_general(query, keys, NT, preferred_element_type=F32) * (
                    1.0 / math.sqrt(HEAD_DIM)
                )
                scores = jnp.where(valid, scores, NEGATIVE)
                sink = sink_ref[h]
                row_top = jnp.maximum(jnp.max(scores, axis=-1, keepdims=True), sink)
                weights = jnp.exp(scores - row_top)
                total = jnp.sum(weights, axis=-1, keepdims=True) + jnp.exp(sink - row_top)
                probs = (weights * (1.0 / total)).astype(BF16)
                mixed.append(jnp.dot(probs, values, preferred_element_type=F32).astype(BF16))
            span = group_size * HEAD_DIM
            mix[rows, pl.ds(g * span, span)] = jnp.concatenate(mixed, axis=1)

    def project(n):
        rows = pl.ds(n * WINDOW, WINDOW)
        projected = jnp.dot(mix[rows, :], out_w[...], preferred_element_type=F32)
        mixer_ref[rows, :] = rms_scale(projected, att_gain_ref[...]).astype(BF16)

    def relay(copy, view):
        copy.wait_recv()
        return [remote(view(far), view(far + j), me_e, t) for j, t in enumerate(mates, 1)]

    for load in load_q[:3]:
        load.wait()
    for n in range(1, blocks):
        attend(n)
    gate_mate = relay(gate_far[0], lambda b: gate_v.at[b, first_rows])
    for copy in rims:
        copy.wait_recv()
    before_at = (before // n_tp, lax.rem(before, n_tp))
    pl.semaphore_signal(ack_sem, inc=1, device_id=before_at, device_id_type=MESH)
    attend(0)
    load_q[3].wait()
    for n in range(blocks):
        project(n)

    def share(side, rows_ref):
        rows = rows_ref[...]
        gate = jnp.dot(rows, common_gate[...], preferred_element_type=F32)
        up = jnp.dot(rows, common_up[...], preferred_element_type=F32)
        units = (silu(gate) * up).astype(BF16)
        shared[side] = jnp.dot(units, common_down[...], preferred_element_type=F32)

    for load in common_loads:
        load.wait()
    for copy in mate_common:
        copy.wait_recv()
    share(0, normed)

    for copy in meta:
        copy.wait_recv()
    normed_far.wait_recv()
    pack(far_ids[...], 1, far_normed)
    share(1, far_normed)

    if merging:
        block = iota((2 * PAIR, tokens), 0)
        over_y, over_x = block // 2, lax.rem(block, 2)
        group = line * PAIR + spot + over_y - 2 * spot * over_y
        for copy in home_meta(0):
            copy.wait_recv()
        route(
            home_ids[...], group * PLANES + plane + over_x - 2 * plane * over_x, home_chosen
        )

        @pl.when(at_end)
        def _():
            empty = pl.ds(pl.multiple_of((1 - upper) * (slots // 2), slots // 2), slots // 2)
            for side in range(2):
                for c in range(CHUNKS):
                    returned[side, c, empty, :] = jnp.zeros((slots // 2, cw), BF16)

    def product(side, weights, low, count):
        rows = arrived[side]
        matrix = weights[low : low + count].reshape(count * width, d)
        return lax.dot_general(rows, matrix, NT, preferred_element_type=F32)

    gate_mate += relay(gate_far[1], lambda b: gate_v.at[b, last_rows])
    for load in own_loads:
        load.wait()
    for copy in mate_kept:
        copy.wait_recv()
    for copy in gate_mate:
        copy.wait_recv()
    wait_rows(0, packed.at[0], arrived.at[0])
    act[0] = silu(product(0, gate_v, 0, 2 * far))
    hidden[0, :, :half] = (act[0, :, :half] * product(0, up_v, 0, far)).astype(BF16)
    up_mate = relay(up_far[0], lambda b: up_v.at[b, up_halves[0]])
    wait_rows(1, packed.at[1], arrived.at[1])
    act[1] = silu(product(1, gate_v, 0, 2 * far))
    hidden[1, :, :half] = (act[1, :, :half] * product(1, up_v, 0, far)).astype(BF16)
    up_mate += relay(up_far[1], lambda b: up_v.at[b, up_halves[1]])
    for copy in up_mate:
        copy.wait_recv()
    for side in range(2):
        hidden[side, :, half:] = (act[side, :, half:] * product(side, up_v, far, far)).astype(BF16)

    def phase(side, c):
        return 2 + side * CHUNKS + c

    eye = iota((tokens, tokens), 0) == iota((tokens, tokens), 1)

    def columns_of(weights):
        return [
            jnp.sum(jnp.where(eye, weights[k : k + 1, :], 0.0), axis=1, keepdims=True)
            for k in range(top)
        ]

    def weigh(total, columns, one_hot, rows):
        picked = lax.dot_general(one_hot, rows, TN, preferred_element_type=F32)
        for k in range(top):
            part = columns[k] * picked[k * tokens : (k + 1) * tokens]
            total = part if total is None else total + part
        return total

    def home_blocks(c):
        routes = (
            (1, home_line * PAIR + spot, me_e, away),
            (0, home_line * PAIR + 1 - spot, pair_e, me_t),
            (1, home_line * PAIR + 1 - spot, pair_e, away),
        )
        return [
            pltpu.make_async_remote_copy(
                outs.at[side, c, rows_of(home)],
                home_rows.at[c, pl.ds(n * cap, cap)],
                home_send.at[c, n],
                home_recv.at[c, n],
                device_id=(e, t),
                device_id_type=MESH,
            )
            for n, (side, home, e, t) in enumerate(routes, 1)
        ]

    def home_step(c):
        to = end_flag * (1 + line // last) + (1 - end_flag) * home_line
        return pltpu.make_async_remote_copy(
            home_out.at[c],
            home_in.at[c],
            home_send.at[c, 0],
            home_recv.at[c, 0],
            device_id=(to * PAIR + spot, me_t),
            device_id_type=MESH,
        )

    def gather_home(c):
        for copy in home_blocks(c):
            copy.start()
        home_rows[c, 0:cap, :] = outs[0, c, rows_of(home_line * PAIR + spot), :]

    def sum_home(c):
        for copy in home_blocks(c):
            copy.wait_recv()
        sums = weigh(None, home_columns, home_chosen[...], home_rows[c])

        @pl.when(at_end)
        def _():
            home_out[c] = sums.astype(BF16)
            home_step(c).start()

        @pl.when(jnp.logical_not(at_end))
        def _():
            home_sums[c] = sums

    def pass_home(c):
        @pl.when(jnp.logical_not(at_end))
        def _():
            home_step(c).wait_recv()
            home_out[c] = (home_sums[c] + home_in[c].astype(F32)).astype(BF16)
            home_step(c).start()

    if merging:
        home_columns = columns_of(home_weight[...])

    def send_back(side, c, first):
        exchange(
            phase(side, c),
            outs.at[side, c],
            returned.at[side, c],
            lambda copy: copy.start(),
            is_sent if merging else None,
            first,
            2,
        )

    for c, cols in enumerate(chunks):
        for copy in relay(down_far[c], lambda b, cols=cols: down_v.at[b, :, cols]):
            copy.wait_recv()
        matrix = down_v[:, :, cols].reshape(2 * half, cw)
        for side in range(2):
            outs[side, c] = jnp.dot(hidden[side], matrix, preferred_element_type=F32).astype(BF16)
        if merging:
            gather_home(c)
        if c + AHEAD < CHUNKS:
            down_far[c + AHEAD].start()
        if merging:
            if c:
                sum_home(c - 1)
            if c == CHUNKS - 1:
                sum_home(c)
        for side in (1, 0):
            send_back(side, c, 2)
            if c < EARLY:
                send_back(side, c, 1)
            keep_rows(outs.at[side, c], returned.at[side, c])
        if merging and c >= 2:
            pass_home(c - 2)
    for c in range(EARLY, CHUNKS):
        for side in (1, 0):
            send_back(side, c, 1)

    scales = [columns_of(weight_ref[...]), columns_of(far_weight[...])]

    def combine(side, c):
        wait_rows(phase(side, c), outs.at[side, c], returned.at[side, c], True)
        return weigh(shared[side, :, chunks[c]], scales[side], chosen[side], returned[side, c])

    parts = []
    for c, cols in enumerate(chunks):
        if merging and c % 2 == 0:
            pass_home(CHUNKS - 2 + c // 2)
        for side in (1, 0):
            if side:
                part_out[c] = combine(1, c).astype(BF16)
                parts.append(remote(part_out.at[c], part_in.at[c], me_e, away))
            else:
                shared[0, :, cols] = combine(0, c)
    if merging:

        @pl.when(at_end)
        def _():
            for c, cols in enumerate(chunks):
                home_step(c).wait_recv()
                shared[0, :, cols] += home_in[c].astype(F32)

    square = jnp.zeros((tokens, 1), F32)
    for c, cols in enumerate(chunks):
        parts[c].wait_recv()
        total = shared[0, :, cols] + part_in[c].astype(F32)
        shared[0, :, cols] = total
        square = square + jnp.sum(total * total, axis=-1, keepdims=True)
    scale = lax.rsqrt(square * (1.0 / d) + EPS)
    experts_ref[...] = (shared[0] * scale * moe_gain_ref[...]).astype(BF16)

    for copy in sent:
        copy.wait_send()
    for side in range(2):
        exchange(side, packed.at[side], arrived.at[side], lambda copy: copy.wait_send())
        for c in range(CHUNKS):
            exchange(
                phase(side, c),
                outs.at[side, c],
                returned.at[side, c],
                lambda copy: copy.wait_send(),
                is_sent if merging else None,
            )
    if merging:
        for c in range(CHUNKS):
            for copy in home_blocks(c) + [home_step(c)]:
                copy.wait_send()

        @pl.when(at_end)
        def _():
            for n in range(2):
                for copy in home_meta(n):
                    copy.wait_send()

    pl.semaphore_wait(ack_sem, 1)


def body(
    att_queries,
    att_keys,
    att_values,
    sink_logits,
    out_weight,
    att_gain,
    moe_in,
    pre_gain,
    expert_ids,
    routed_expert_weight,
    w_gate,
    w_up,
    w_down,
    common_expert_gate_weight,
    common_expert_up_weight,
    common_expert_down_weight,
    moe_gain,
):
    assert w_gate.shape[0] == PLANES
    n_ep, n_tp = lax.axis_size("ep"), lax.axis_size("tp")
    rows, width = att_queries.shape
    tokens, d = moe_in.shape
    top = expert_ids.shape[1]
    slot_cap = 2 * tokens * top // (PLANES * n_ep)
    cap = -(-slot_cap // ROW_TILE) * ROW_TILE
    slots = cap * n_ep
    far = n_tp // PLANES
    blocks = 2 * far
    kv = att_keys.shape[1]
    units = w_gate.shape[2]
    common = common_expert_gate_weight.shape[1]
    cw = d // CHUNKS
    scratch = [
        pltpu.VMEM((tokens, d), BF16),
        pltpu.VMEM((tokens, d), BF16),
        pltpu.VMEM((tokens, d), BF16),
        pltpu.VMEM((top, tokens), jnp.int32),
        pltpu.VMEM((top, tokens), F32),
        pltpu.VMEM((2, slots, top * tokens), BF16),
        pltpu.VMEM((2, slots, d), BF16),
        pltpu.VMEM((2, slots, d), BF16),
        pltpu.VMEM((2, CHUNKS, slots, cw), BF16),
        pltpu.VMEM((2, CHUNKS, slots, cw), BF16),
        pltpu.VMEM((blocks, units, d), BF16),
        pltpu.VMEM((blocks, units, d), BF16),
        pltpu.VMEM((blocks, units, d), BF16),
        pltpu.VMEM((2, slots, blocks * units), F32),
        pltpu.VMEM((2, slots, blocks * units), BF16),
        pltpu.VMEM((d, far * common), BF16),
        pltpu.VMEM((d, far * common), BF16),
        pltpu.VMEM((far * common, d), BF16),
        pltpu.VMEM((2, tokens, d), F32),
        pltpu.VMEM((CHUNKS, tokens, cw), BF16),
        pltpu.VMEM((CHUNKS, tokens, cw), BF16),
        pltpu.VMEM((rows, width), BF16),
        pltpu.VMEM((rows, kv), BF16),
        pltpu.VMEM((rows, kv), BF16),
        pltpu.VMEM((WINDOW, kv), BF16),
        pltpu.VMEM((WINDOW, kv), BF16),
        pltpu.VMEM(out_weight.shape, BF16),
        pltpu.VMEM((rows, width), BF16),
        pltpu.SemaphoreType.DMA((11,)),
        pltpu.SemaphoreType.DMA((9 + 2 * CHUNKS + (far - 1) * (10 + CHUNKS),)),
        pltpu.SemaphoreType.DMA((9 + 2 * CHUNKS + (far - 1) * (10 + CHUNKS),)),
        pltpu.SemaphoreType.DMA((2 + 2 * CHUNKS, n_ep)),
        pltpu.SemaphoreType.DMA((2 + 2 * CHUNKS, n_ep)),
        pltpu.SemaphoreType.REGULAR,
    ]
    if n_ep == PAIR * LINE and far == 2:
        scratch += [
            pltpu.VMEM((top, tokens), jnp.int32),
            pltpu.VMEM((top, tokens), F32),
            pltpu.VMEM((2 * PAIR * cap, top * tokens), BF16),
            pltpu.VMEM((CHUNKS, 2 * PAIR * cap, cw), BF16),
            pltpu.VMEM((CHUNKS, tokens, cw), F32),
            pltpu.VMEM((CHUNKS, tokens, cw), BF16),
            pltpu.VMEM((CHUNKS, tokens, cw), BF16),
            pltpu.SemaphoreType.DMA((2, 2)),
            pltpu.SemaphoreType.DMA((2,)),
            pltpu.SemaphoreType.DMA((CHUNKS, 4)),
            pltpu.SemaphoreType.DMA((CHUNKS, 4)),
        ]
    return pl.pallas_call(
        functools.partial(layer_kernel, n_ep, n_tp, cap),
        out_shape=(
            pltpu.VMEM((rows, d), BF16),
            pltpu.VMEM((tokens, d), BF16),
        ),
        in_specs=[SMEM] + [VMEM] * 5 + [ANY] * 11,
        out_specs=(VMEM, VMEM),
        scratch_shapes=scratch,
        compiler_params=pltpu.CompilerParams(
            vmem_limit_bytes=62 * 1024 * 1024 + 256 * 1024, collective_id=0, has_side_effects=True
        ),
        name="layer",
    )(
        sink_logits,
        expert_ids.T,
        routed_expert_weight.T,
        pre_gain[None],
        att_gain[None],
        moe_gain[None],
        att_queries,
        att_keys,
        att_values,
        out_weight,
        moe_in,
        jnp.swapaxes(w_gate, 1, 2),
        jnp.swapaxes(w_up, 1, 2),
        w_down,
        common_expert_gate_weight,
        common_expert_up_weight,
        common_expert_down_weight,
    )


def solution(mesh):
    tokens_spec = P(("ep", "tp"), None)
    in_specs = (
        tokens_spec,
        tokens_spec,
        tokens_spec,
        P(),
        P(),
        P(),
        tokens_spec,
        P(),
        tokens_spec,
        tokens_spec,
        P("ep", None, "tp"),
        P("ep", None, "tp"),
        P("ep", "tp", None),
        P(None, "tp"),
        P(None, "tp"),
        P("tp", None),
        P(),
    )
    return jax.shard_map(
        body, mesh=mesh, in_specs=in_specs, out_specs=(tokens_spec, tokens_spec), check_vma=False
    )
```

```python
import functools
import math

import jax
import jax.numpy as jnp
from jax import lax
from jax.experimental import pallas as pl
from jax.experimental.pallas import tpu as pltpu
from jax.sharding import PartitionSpec as P

HEADS = 16
KV_HEADS = 4
HEAD_DIM = 64
WINDOW = 128

EPS = 1e-06
NEGATIVE = -1e30
PLANES = 2
WIDTHS = (2, 4, 4, 4, 2)
CHUNKS = len(WIDTHS)
AHEAD = 2
EARLY = 2
ROW_TILE = 8
PAIR = 2
LINE = 4

VMEM = pl.BlockSpec(memory_space=pltpu.VMEM)
SMEM = pl.BlockSpec(memory_space=pltpu.SMEM)
ANY = pl.BlockSpec(memory_space=pl.ANY)
F32 = jnp.float32
BF16 = jnp.bfloat16
MESH = pl.DeviceIdType.MESH
NT = (((1,), (1,)), ((), ()))
TN = (((0,), (0,)), ((), ()))


def iota(shape, dim):
    return lax.broadcasted_iota(jnp.int32, shape, dim)


def rms_scale(inputs, gain_vec):
    mean_sq = jnp.mean(inputs * inputs, axis=-1, keepdims=True)
    return inputs * lax.rsqrt(mean_sq + EPS) * gain_vec


def silu(v):
    return v / (1.0 + jnp.exp(-v))


def flip(index, amount):
    bit = 1
    while bit <= amount:
        if amount & bit:
            index = index + bit - 2 * bit * lax.rem(index // bit, 2)
        bit *= 2
    return index


class Sems:
    def __init__(self, *arrays):
        self.arrays, self.used = arrays, 0

    def take(self):
        self.used += 1
        return [array.at[self.used - 1] for array in self.arrays]


def layer_kernel(
    n_ep,
    n_tp,
    cap,
    sink_ref,
    ids_ref,
    weight_ref,
    pre_gain_ref,
    att_gain_ref,
    moe_gain_ref,
    q_hbm,
    k_hbm,
    v_hbm,
    out_w_hbm,
    x_hbm,
    gate_hbm,
    up_hbm,
    down_hbm,
    common_gate_hbm,
    common_up_hbm,
    common_down_hbm,
    mixer_ref,
    experts_ref,
    x_v,
    normed,
    far_normed,
    far_ids,
    far_weight,
    chosen,
    packed,
    arrived,
    outs,
    returned,
    gate_v,
    up_v,
    down_v,
    act,
    hidden,
    common_gate,
    common_up,
    common_down,
    shared,
    part_out,
    part_in,
    q_v,
    k_v,
    v_v,
    rim_k,
    rim_v,
    out_w,
    mix,
    local_sems,
    send_sems,
    recv_sems,
    row_send,
    row_recv,
    ack_sem,
    *merge_refs,
):
    far = n_tp // PLANES
    tokens, d = x_v.shape
    top = ids_ref.shape[0]
    merging = bool(merge_refs)
    if merging:
        (
            home_ids,
            home_weight,
            home_chosen,
            home_rows,
            home_sums,
            home_out,
            home_in,
            meta_send,
            meta_recv,
            home_send,
            home_recv,
        ) = merge_refs
    slots = n_ep * cap
    width = gate_hbm.shape[1]
    half = far * width
    unit = d // sum(WIDTHS)
    me_e, me_t = lax.axis_index("ep"), lax.axis_index("tp")
    plane = me_t // far
    away = flip(me_t, far)
    mates = [flip(me_t, j) for j in range(1, far)]
    devices = n_ep * n_tp
    me = me_e * n_tp + me_t
    after, before = lax.rem(me + 1, devices), lax.rem(me + devices - 1, devices)
    local, net, shared_sends = Sems(local_sems), Sems(recv_sems), Sems(send_sems)

    line, spot = me_e // PAIR, lax.rem(me_e, PAIR)
    last = LINE - 1
    upper = line // (LINE // 2)
    home_line = last * (1 - upper)
    at_end = lax.rem(line, last) == 0
    end_flag = 1 - (lax.rem(line, last) + 1) // 2
    pair_e = line * PAIR + 1 - spot
    sent = {}

    def fetch(src, dst):
        copy = pltpu.make_async_copy(src, dst, local.take()[0])
        copy.start()
        return copy

    def remote(src, dst, e, t, name, start=True):
        if name not in sent:
            sent[name] = shared_sends.take()[0]
        copy = pltpu.make_async_remote_copy(
            src, dst, sent[name], net.take()[0], device_id=(e, t), device_id_type=MESH
        )
        if start:
            copy.start()
        return copy

    def settle(name, ref):
        pltpu.make_async_remote_copy(
            ref, ref, sent.pop(name), recv_sems.at[0], device_id=(me_e, away), device_id_type=MESH
        ).wait_send()

    def rows_of(group):
        return pl.ds(pl.multiple_of(group * cap, cap), cap)

    def exchange(phase, src, dst, cols, wanted=None, first=1, stride=1):
        def step(i, carry):
            j = first + stride * i
            to = lax.rem(me_e + j, n_ep)
            copy = pltpu.make_async_remote_copy(
                src.at[rows_of(to), cols],
                dst.at[rows_of(me_e), cols],
                row_send.at[min(phase, 2) // 2],
                row_recv.at[phase],
                device_id=(to, me_t),
                device_id_type=MESH,
            )
            if wanted is None:
                copy.start()
            else:
                pl.when(wanted(j))(lambda: copy.start())
            return carry

        lax.fori_loop(0, (n_ep - first + stride - 1) // stride, step, 0)

    def wait_rows(phase, dst, cols, peers):
        view = dst.at[pl.ds(0, peers * cap), cols]
        pltpu.make_async_remote_copy(
            view,
            view,
            row_send.at[0],
            row_recv.at[phase],
            device_id=(me_e, away),
            device_id_type=MESH,
        ).wait_recv()

    def wait_sent(kind, src, peers):
        view = src.at[:, pl.ds(0, peers * cap)]
        pltpu.make_async_remote_copy(
            view,
            view,
            row_send.at[kind],
            row_recv.at[0],
            device_id=(me_e, away),
            device_id_type=MESH,
        ).wait_send()

    def is_sent(j):
        return lax.rem(me_e + j, n_ep) // PAIR != home_line

    def keep_rows(src, dst, cols):
        dst[rows_of(me_e), cols] = src[rows_of(me_e), cols]

    everything = pl.ds(0, d)

    def wait_dispatch(side):
        wait_rows(side, arrived.at[side], everything, n_ep - 1)

    load_x = fetch(x_hbm, x_v)
    barrier = pltpu.get_barrier_semaphore()

    def greet(j, carry):
        pl.semaphore_signal(
            barrier, inc=1, device_id=(lax.rem(me_e + j, n_ep), me_t), device_id_type=MESH
        )
        return carry

    lax.fori_loop(1, n_ep, greet, 0)
    for t in [away] + mates:
        pl.semaphore_signal(barrier, inc=1, device_id=(me_e, t), device_id_type=MESH)
    for n in (after, before):
        pl.semaphore_signal(
            barrier, inc=1, device_id=(n // n_tp, lax.rem(n, n_tp)), device_id_type=MESH
        )
    if merging:
        pl.semaphore_signal(barrier, inc=1, device_id=(pair_e, away), device_id_type=MESH)
    own_loads = []
    for src, dst in ((gate_hbm, gate_v), (up_hbm, up_v), (down_hbm, down_v)):
        own_loads.append(fetch(src.at[plane], dst.at[0]))
    load_q = [fetch(q_hbm, q_v), fetch(k_hbm, k_v), fetch(v_hbm, v_v), fetch(out_w_hbm, out_w)]
    common_cols = common_gate_hbm.shape[1]
    common_loads = [
        fetch(common_gate_hbm, common_gate.at[:, pl.ds(0, common_cols)]),
        fetch(common_up_hbm, common_up.at[:, pl.ds(0, common_cols)]),
        fetch(common_down_hbm, common_down.at[pl.ds(0, common_cols)]),
    ]
    pl.semaphore_wait(barrier, n_ep - 1 + far + 2 + int(merging))

    cut = width // 4
    first_rows, last_rows = pl.ds(0, cut), pl.ds(cut, width - cut)
    other = PLANES - 1 - plane
    gate_far = [
        remote(gate_hbm.at[other, first_rows], gate_v.at[far, first_rows], me_e, away, "gate"),
    ]
    meta = [
        remote(ids_ref, far_ids, me_e, away, "ids"),
        remote(weight_ref, far_weight, me_e, away, "weight"),
    ]
    mate_common, mate_kept = [], []
    for j, t in enumerate(mates, 1):
        cols = pl.ds(j * common_cols, common_cols)
        for kind, (src, dst) in enumerate(
            (
                (common_gate_hbm, common_gate.at[:, cols]),
                (common_up_hbm, common_up.at[:, cols]),
                (common_down_hbm, common_down.at[cols]),
            )
        ):
            mate_common.append(remote(src, dst, me_e, t, ("common", kind, j)))
    edge = k_hbm.shape[0] - WINDOW
    after_at = (after // n_tp, lax.rem(after, n_tp))
    rims = [
        remote(k_hbm.at[pl.ds(edge, WINDOW)], rim_k, *after_at, "rim_k", False),
        remote(v_hbm.at[pl.ds(edge, WINDOW)], rim_v, *after_at, "rim_v", False),
    ]

    def home_meta(n):
        lines = (LINE // 2 - upper, last - line)
        to = lines[n] * PAIR + spot
        return [
            pltpu.make_async_remote_copy(
                src,
                dst,
                meta_send.at[n, i],
                meta_recv.at[i],
                device_id=(to, me_t),
                device_id_type=MESH,
            )
            for i, (src, dst) in enumerate(((ids_ref, home_ids), (weight_ref, home_weight)))
        ]

    if merging:

        @pl.when(at_end)
        def _():
            for n in range(2):
                for copy in home_meta(n):
                    copy.start()

    load_x.wait()
    normed[...] = rms_scale(x_v[...].astype(F32), pre_gain_ref[...]).astype(BF16)
    normed_far = remote(normed, far_normed, me_e, away, "normed")
    gate_far.append(
        remote(gate_hbm.at[other, last_rows], gate_v.at[far, last_rows], me_e, away, "gate")
    )
    up_halves = [pl.ds(0, width // 2), pl.ds(width // 2, width // 2)]
    up_far = [
        remote(up_hbm.at[other, rows], up_v.at[far, rows], me_e, away, "up") for rows in up_halves
    ]
    chunks = [pl.ds(sum(WIDTHS[:c]) * unit, WIDTHS[c] * unit) for c in range(CHUNKS)]
    down_far = [
        remote(
            down_hbm.at[other, :, cols], down_v.at[far, :, cols], me_e, away, "down", c < AHEAD
        )
        for c, cols in enumerate(chunks)
    ]

    earlier = (iota((tokens, tokens), 0) < iota((tokens, tokens), 1)).astype(F32).astype(BF16)

    def route(ids, numbers, chosen_ref):
        hits = [numbers == ids[k : k + 1, :] for k in range(top)]
        hit = functools.reduce(lambda a, b: a | b, hits).astype(F32).astype(BF16)
        count = jnp.dot(hit, earlier, preferred_element_type=F32)
        place = count + (iota(numbers.shape, 0) * cap + 1).astype(F32)
        slot_number = (iota((chosen_ref.shape[0], tokens), 0) + 1).astype(F32)
        total = None
        for k in range(top):
            slot = jnp.sum(jnp.where(hits[k], place, 0.0), axis=0, keepdims=True)
            one_hot = (slot_number == slot).astype(F32).astype(BF16)
            chosen_ref[:, k * tokens : (k + 1) * tokens] = one_hot
            total = one_hot if total is None else total + one_hot
        return total

    def pack(ids, side, rows_ref):
        numbers = iota((n_ep, tokens), 0) * PLANES + plane
        one_hot = route(ids, numbers, chosen.at[side])
        rows = rows_ref[...]
        step = slots // 2
        for i in range(2):
            packed[side, i * step : (i + 1) * step, :] = jnp.dot(
                one_hot[i * step : (i + 1) * step], rows, preferred_element_type=F32
            ).astype(BF16)
        exchange(side, packed.at[side], arrived.at[side], everything)
        keep_rows(packed.at[side], arrived.at[side], everything)

    pack(ids_ref[...], 0, normed)
    for j, t in enumerate(mates, 1):
        for kind, (src, dst) in enumerate(
            ((gate_hbm, gate_v), (up_hbm, up_v), (down_hbm, down_v))
        ):
            mate_kept.append(remote(src.at[plane], dst.at[j], me_e, t, ("kept", kind, j)))

    group_size = HEADS // KV_HEADS
    blocks = q_v.shape[0] // WINDOW
    shape = (WINDOW, 2 * WINDOW)
    gap = iota(shape, 0) + WINDOW - iota(shape, 1)
    inside = (gap >= 0) & (gap < WINDOW)

    def attend(n):
        rows = pl.ds(n * WINDOW, WINDOW)
        valid = inside
        if n == 0:
            valid = inside & (iota(shape, 1) + me * q_v.shape[0] >= WINDOW)
        for g in range(KV_HEADS):
            cols = pl.ds(g * HEAD_DIM, HEAD_DIM)
            if n == 0:
                keys = jnp.concatenate([rim_k[:, cols], k_v[rows, cols]], axis=0)
                values = jnp.concatenate([rim_v[:, cols], v_v[rows, cols]], axis=0)
            else:
                band = pl.ds((n - 1) * WINDOW, 2 * WINDOW)
                keys, values = k_v[band, cols], v_v[band, cols]
            mixed = []
            for j in range(group_size):
                h = g * group_size + j
                query = q_v[rows, pl.ds(h * HEAD_DIM, HEAD_DIM)]
                scores = lax.dot_general(query, keys, NT, preferred_element_type=F32) * (
                    1.0 / math.sqrt(HEAD_DIM)
                )
                scores = jnp.where(valid, scores, NEGATIVE)
                sink = sink_ref[h]
                row_top = jnp.maximum(jnp.max(scores, axis=-1, keepdims=True), sink)
                weights = jnp.exp(scores - row_top)
                total = jnp.sum(weights, axis=-1, keepdims=True) + jnp.exp(sink - row_top)
                probs = (weights * (1.0 / total)).astype(BF16)
                mixed.append(jnp.dot(probs, values, preferred_element_type=F32).astype(BF16))
            span = group_size * HEAD_DIM
            mix[rows, pl.ds(g * span, span)] = jnp.concatenate(mixed, axis=1)

    def project(n):
        rows = pl.ds(n * WINDOW, WINDOW)
        projected = jnp.dot(mix[rows, :], out_w[...], preferred_element_type=F32)
        mixer_ref[rows, :] = rms_scale(projected, att_gain_ref[...]).astype(BF16)

    def relay(copy, view, kind):
        copy.wait_recv()
        return [
            remote(view(far), view(far + j), me_e, t, ("relay", kind, j))
            for j, t in enumerate(mates, 1)
        ]

    for load in load_q[:3]:
        load.wait()
    for n in range(1, blocks):
        attend(n)
    gate_mate = relay(gate_far[0], lambda b: gate_v.at[b, first_rows], 0)
    load_q[3].wait()
    for n in range(1, blocks):
        project(n)

    def attend_rim():
        for copy in rims:
            copy.wait_recv()
        before_at = (before // n_tp, lax.rem(before, n_tp))
        pl.semaphore_signal(ack_sem, inc=1, device_id=before_at, device_id_type=MESH)
        attend(0)
        project(0)

    def share(side, rows_ref):
        rows = rows_ref[...]
        gate = jnp.dot(rows, common_gate[...], preferred_element_type=F32)
        up = jnp.dot(rows, common_up[...], preferred_element_type=F32)
        units = (silu(gate) * up).astype(BF16)
        shared[side] = jnp.dot(units, common_down[...], preferred_element_type=F32)

    for load in common_loads:
        load.wait()
    for copy in mate_common:
        copy.wait_recv()
    share(0, normed)

    for copy in meta:
        copy.wait_recv()
    normed_far.wait_recv()
    pack(far_ids[...], 1, far_normed)
    share(1, far_normed)

    if merging:
        block = iota((2 * PAIR, tokens), 0)
        over_y, over_x = block // 2, lax.rem(block, 2)
        group = line * PAIR + spot + over_y - 2 * spot * over_y
        for copy in home_meta(0):
            copy.wait_recv()
        route(
            home_ids[...], group * PLANES + plane + over_x - 2 * plane * over_x, home_chosen
        )

        @pl.when(at_end)
        def _():
            empty = pl.ds(pl.multiple_of((1 - upper) * (slots // 2), slots // 2), slots // 2)
            for side in range(2):
                returned[side, empty, :] = jnp.zeros((slots // 2, d), BF16)

    def product(side, weights, low, count):
        rows = arrived[side]
        matrix = weights[low : low + count].reshape(count * width, d)
        return lax.dot_general(rows, matrix, NT, preferred_element_type=F32)

    gate_mate += relay(gate_far[1], lambda b: gate_v.at[b, last_rows], 0)
    for load in own_loads:
        load.wait()
    for copy in mate_kept:
        copy.wait_recv()
    for copy in gate_mate:
        copy.wait_recv()
    wait_dispatch(0)
    act[0] = silu(product(0, gate_v, 0, 2 * far))
    hidden[0, :, :half] = (act[0, :, :half] * product(0, up_v, 0, far)).astype(BF16)
    up_mate = relay(up_far[0], lambda b: up_v.at[b, up_halves[0]], 1)
    up_mate += relay(up_far[1], lambda b: up_v.at[b, up_halves[1]], 1)
    wait_dispatch(1)
    act[1] = silu(product(1, gate_v, 0, 2 * far))
    hidden[1, :, :half] = (act[1, :, :half] * product(1, up_v, 0, far)).astype(BF16)

    def relay_down(c):
        cols = chunks[c]
        return relay(down_far[c], lambda b: down_v.at[b, :, cols], 2)

    down_mate = relay_down(0)
    for copy in up_mate:
        copy.wait_recv()
    for side in range(2):
        hidden[side, :, half:] = (act[side, :, half:] * product(side, up_v, far, far)).astype(BF16)

    def phase(side, c):
        return 2 + side * CHUNKS + c

    eye = iota((tokens, tokens), 0) == iota((tokens, tokens), 1)

    def columns_of(weights):
        return [
            jnp.sum(jnp.where(eye, weights[k : k + 1, :], 0.0), axis=1, keepdims=True)
            for k in range(top)
        ]

    def weigh(total, columns, one_hot, rows):
        picked = lax.dot_general(one_hot, rows, TN, preferred_element_type=F32)
        for k in range(top):
            part = columns[k] * picked[k * tokens : (k + 1) * tokens]
            total = part if total is None else total + part
        return total

    def home_blocks(c):
        routes = (
            (1, home_line * PAIR + spot, me_e, away),
            (0, home_line * PAIR + 1 - spot, pair_e, me_t),
            (1, home_line * PAIR + 1 - spot, pair_e, away),
        )
        return [
            pltpu.make_async_remote_copy(
                outs.at[side, rows_of(home), chunks[c]],
                home_rows.at[pl.ds(n * cap, cap), chunks[c]],
                home_send.at[1],
                home_recv.at[c, 1],
                device_id=(e, t),
                device_id_type=MESH,
            )
            for n, (side, home, e, t) in enumerate(routes, 1)
        ]

    def home_step(c):
        to = end_flag * (1 + line // last) + (1 - end_flag) * home_line
        return pltpu.make_async_remote_copy(
            home_out.at[:, chunks[c]],
            home_in.at[:, chunks[c]],
            home_send.at[0],
            home_recv.at[c, 0],
            device_id=(to * PAIR + spot, me_t),
            device_id_type=MESH,
        )

    def gather_home(c):
        for copy in home_blocks(c):
            copy.start()
        home_rows[0:cap, chunks[c]] = outs[0, rows_of(home_line * PAIR + spot), chunks[c]]

    def sum_home(c):
        view = home_rows.at[pl.ds(0, (2 * PAIR - 1) * cap), chunks[c]]
        pltpu.make_async_remote_copy(
            view,
            view,
            home_send.at[1],
            home_recv.at[c, 1],
            device_id=(me_e, away),
            device_id_type=MESH,
        ).wait_recv()
        sums = weigh(None, home_columns, home_chosen[...], home_rows[:, chunks[c]])

        @pl.when(at_end)
        def _():
            home_out[:, chunks[c]] = sums.astype(BF16)
            home_step(c).start()

        @pl.when(jnp.logical_not(at_end))
        def _():
            home_sums[:, chunks[c]] = sums

    def pass_home(c):
        @pl.when(jnp.logical_not(at_end))
        def _():
            home_step(c).wait_recv()
            sums = home_sums[:, chunks[c]] + home_in[:, chunks[c]].astype(F32)
            home_out[:, chunks[c]] = sums.astype(BF16)
            home_step(c).start()

    if merging:
        home_columns = columns_of(home_weight[...])

    def send_back(side, c, first):
        exchange(
            phase(side, c),
            outs.at[side],
            returned.at[side],
            chunks[c],
            is_sent if merging else None,
            first,
            2,
        )

    for c, cols in enumerate(chunks):
        if c:
            down_mate = relay_down(c)
        for copy in down_mate:
            copy.wait_recv()
        matrix = down_v[:, :, cols].reshape(2 * half, WIDTHS[c] * unit)
        for side in range(2):
            outs[side, :, cols] = jnp.dot(hidden[side], matrix, preferred_element_type=F32).astype(BF16)
        if merging:
            gather_home(c)
        if c + AHEAD < CHUNKS:
            down_far[c + AHEAD].start()
        if c + AHEAD == CHUNKS:
            for copy in rims:
                copy.start()
        if merging:
            if c:
                sum_home(c - 1)
            if c == CHUNKS - 1:
                sum_home(c)
        for side in (1, 0):
            send_back(side, c, 2)
            if c < EARLY:
                send_back(side, c, 1)
            keep_rows(outs.at[side], returned.at[side], cols)
        if merging and c >= 2:
            pass_home(c - 2)
    for c in range(EARLY, CHUNKS):
        for side in (1, 0):
            send_back(side, c, 1)

    scales = [columns_of(weight_ref[...]), columns_of(far_weight[...])]

    def wait_back(side, c):
        if not merging:
            wait_rows(phase(side, c), returned.at[side], chunks[c], n_ep - 1)
            return

        @pl.when(at_end)
        def _():
            wait_rows(phase(side, c), returned.at[side], chunks[c], n_ep // 2 - 1)

        @pl.when(jnp.logical_not(at_end))
        def _():
            wait_rows(phase(side, c), returned.at[side], chunks[c], n_ep - 1)

    def combine(side, c):
        wait_back(side, c)
        cols = chunks[c]
        return weigh(shared[side, :, cols], scales[side], chosen[side], returned[side, :, cols])

    parts = []
    for c, cols in enumerate(chunks):
        if merging and c == 0:
            pass_home(CHUNKS - 2)
        if merging and c == EARLY:
            pass_home(CHUNKS - 1)
        if c == EARLY:
            attend_rim()
        part_out[:, cols] = combine(1, c).astype(BF16)
        parts.append(remote(part_out.at[:, cols], part_in.at[:, cols], me_e, away, "part"))
        shared[0, :, cols] = combine(0, c)

    wait_sent(0, packed, n_ep - 1)
    wait_sent(1, outs, n_ep - 1 - (PAIR if merging else 0))
    settle("ids", ids_ref)
    settle("weight", weight_ref)
    settle("normed", normed)
    settle("rim_k", rim_k)
    settle("rim_v", rim_v)
    for name, ref in (("gate", gate_hbm), ("up", up_hbm), ("down", down_hbm)):
        settle(name, ref.at[other])
    for j in range(1, far):
        for kind, ref in enumerate((gate_v, up_v, down_v)):
            settle(("kept", kind, j), ref.at[0])
            settle(("relay", kind, j), ref.at[far])
        for kind, ref in enumerate((common_gate_hbm, common_up_hbm, common_down_hbm)):
            settle(("common", kind, j), ref)
    if merging:
        for n, view in enumerate((home_out, home_rows.at[pl.ds(0, (2 * PAIR - 1) * cap)])):
            pltpu.make_async_remote_copy(
                view,
                view,
                home_send.at[n],
                home_recv.at[0, 0],
                device_id=(me_e, away),
                device_id_type=MESH,
            ).wait_send()
    pl.semaphore_wait(ack_sem, 1)
    if merging:

        @pl.when(at_end)
        def _():
            for n in range(2):
                for copy in home_meta(n):
                    copy.wait_send()

    square = jnp.zeros((tokens, 1), F32)
    for c, cols in enumerate(chunks):
        if merging:

            @pl.when(at_end)
            def _():
                home_step(c).wait_recv()
                shared[0, :, cols] += home_in[:, cols].astype(F32)

        parts[c].wait_recv()
        total = shared[0, :, cols] + part_in[:, cols].astype(F32)
        shared[0, :, cols] = total
        square = square + jnp.sum(total * total, axis=-1, keepdims=True)
    scale = lax.rsqrt(square * (1.0 / d) + EPS)
    experts_ref[...] = (shared[0] * scale * moe_gain_ref[...]).astype(BF16)
    settle("part", part_out)
    assert not sent


def body(
    att_queries,
    att_keys,
    att_values,
    sink_logits,
    out_weight,
    att_gain,
    moe_in,
    pre_gain,
    expert_ids,
    routed_expert_weight,
    w_gate,
    w_up,
    w_down,
    common_expert_gate_weight,
    common_expert_up_weight,
    common_expert_down_weight,
    moe_gain,
):
    assert w_gate.shape[0] == PLANES
    n_ep, n_tp = lax.axis_size("ep"), lax.axis_size("tp")
    rows, width = att_queries.shape
    tokens, d = moe_in.shape
    top = expert_ids.shape[1]
    slot_cap = 2 * tokens * top // (PLANES * n_ep)
    cap = -(-slot_cap // ROW_TILE) * ROW_TILE
    slots = cap * n_ep
    far = n_tp // PLANES
    blocks = 2 * far
    kv = att_keys.shape[1]
    units = w_gate.shape[2]
    common = common_expert_gate_weight.shape[1]
    scratch = [
        pltpu.VMEM((tokens, d), BF16),
        pltpu.VMEM((tokens, d), BF16),
        pltpu.VMEM((tokens, d), BF16),
        pltpu.VMEM((top, tokens), jnp.int32),
        pltpu.VMEM((top, tokens), F32),
        pltpu.VMEM((2, slots, top * tokens), BF16),
        pltpu.VMEM((2, slots, d), BF16),
        pltpu.VMEM((2, slots, d), BF16),
        pltpu.VMEM((2, slots, d), BF16),
        pltpu.VMEM((2, slots, d), BF16),
        pltpu.VMEM((blocks, units, d), BF16),
        pltpu.VMEM((blocks, units, d), BF16),
        pltpu.VMEM((blocks, units, d), BF16),
        pltpu.VMEM((2, slots, blocks * units), F32),
        pltpu.VMEM((2, slots, blocks * units), BF16),
        pltpu.VMEM((d, far * common), BF16),
        pltpu.VMEM((d, far * common), BF16),
        pltpu.VMEM((far * common, d), BF16),
        pltpu.VMEM((2, tokens, d), F32),
        pltpu.VMEM((tokens, d), BF16),
        pltpu.VMEM((tokens, d), BF16),
        pltpu.VMEM((rows, width), BF16),
        pltpu.VMEM((rows, kv), BF16),
        pltpu.VMEM((rows, kv), BF16),
        pltpu.VMEM((WINDOW, kv), BF16),
        pltpu.VMEM((WINDOW, kv), BF16),
        pltpu.VMEM(out_weight.shape, BF16),
        pltpu.VMEM((rows, width), BF16),
        pltpu.SemaphoreType.DMA((11,)),
        pltpu.SemaphoreType.DMA((9 + (far - 1) * 9,)),
        pltpu.SemaphoreType.DMA((9 + 2 * CHUNKS + (far - 1) * (10 + CHUNKS),)),
        pltpu.SemaphoreType.DMA((2,)),
        pltpu.SemaphoreType.DMA((2 + 2 * CHUNKS,)),
        pltpu.SemaphoreType.REGULAR,
    ]
    if n_ep == PAIR * LINE and far == 2:
        scratch += [
            pltpu.VMEM((top, tokens), jnp.int32),
            pltpu.VMEM((top, tokens), F32),
            pltpu.VMEM((2 * PAIR * cap, top * tokens), BF16),
            pltpu.VMEM((2 * PAIR * cap, d), BF16),
            pltpu.VMEM((tokens, d), F32),
            pltpu.VMEM((tokens, d), BF16),
            pltpu.VMEM((tokens, d), BF16),
            pltpu.SemaphoreType.DMA((2, 2)),
            pltpu.SemaphoreType.DMA((2,)),
            pltpu.SemaphoreType.DMA((2,)),
            pltpu.SemaphoreType.DMA((CHUNKS, 2)),
        ]
    return pl.pallas_call(
        functools.partial(layer_kernel, n_ep, n_tp, cap),
        out_shape=(
            pltpu.VMEM((rows, d), BF16),
            pltpu.VMEM((tokens, d), BF16),
        ),
        in_specs=[SMEM] + [VMEM] * 5 + [ANY] * 11,
        out_specs=(VMEM, VMEM),
        scratch_shapes=scratch,
        compiler_params=pltpu.CompilerParams(
            vmem_limit_bytes=62 * 1024 * 1024 + 256 * 1024, collective_id=0, has_side_effects=True
        ),
        name="layer",
    )(
        sink_logits,
        expert_ids.T,
        routed_expert_weight.T,
        pre_gain[None],
        att_gain[None],
        moe_gain[None],
        att_queries,
        att_keys,
        att_values,
        out_weight,
        moe_in,
        jnp.swapaxes(w_gate, 1, 2),
        jnp.swapaxes(w_up, 1, 2),
        w_down,
        common_expert_gate_weight,
        common_expert_up_weight,
        common_expert_down_weight,
    )


def solution(mesh):
    tokens_spec = P(("ep", "tp"), None)
    in_specs = (
        tokens_spec,
        tokens_spec,
        tokens_spec,
        P(),
        P(),
        P(),
        tokens_spec,
        P(),
        tokens_spec,
        tokens_spec,
        P("ep", None, "tp"),
        P("ep", None, "tp"),
        P("ep", "tp", None),
        P(None, "tp"),
        P(None, "tp"),
        P("tp", None),
        P(),
    )
    return jax.shard_map(
        body, mesh=mesh, in_specs=in_specs, out_specs=(tokens_spec, tokens_spec), check_vma=False
    )
```

```python
import functools
import math

import jax
import jax.numpy as jnp
from jax import lax
from jax.experimental import pallas as pl
from jax.experimental.pallas import tpu as pltpu
from jax.sharding import PartitionSpec as P

HEADS = 16
KV_HEADS = 4
HEAD_DIM = 64
WINDOW = 128

EPS = 1e-06
NEGATIVE = -1e30
PLANES = 2
WIDTHS = (2, 4, 4, 4, 2)
CHUNKS = len(WIDTHS)
AHEAD = 2
EARLY = 2
ROW_TILE = 8
PAIR = 2
LINE = 4

VMEM = pl.BlockSpec(memory_space=pltpu.VMEM)
SMEM = pl.BlockSpec(memory_space=pltpu.SMEM)
ANY = pl.BlockSpec(memory_space=pl.ANY)
F32 = jnp.float32
BF16 = jnp.bfloat16
MESH = pl.DeviceIdType.MESH
NT = (((1,), (1,)), ((), ()))
TN = (((0,), (0,)), ((), ()))


def iota(shape, dim):
    return lax.broadcasted_iota(jnp.int32, shape, dim)


def rms_scale(inputs, gain_vec):
    mean_sq = jnp.mean(inputs * inputs, axis=-1, keepdims=True)
    return inputs * lax.rsqrt(mean_sq + EPS) * gain_vec


def silu(v):
    return v / (1.0 + jnp.exp(-v))


def flip(index, amount):
    bit = 1
    while bit <= amount:
        if amount & bit:
            index = index + bit - 2 * bit * lax.rem(index // bit, 2)
        bit *= 2
    return index


class Sems:
    def __init__(self, *arrays):
        self.arrays, self.used = arrays, 0

    def take(self):
        self.used += 1
        return [array.at[self.used - 1] for array in self.arrays]


def layer_kernel(
    n_ep,
    n_tp,
    cap,
    sink_ref,
    ids_ref,
    weight_ref,
    pre_gain_ref,
    att_gain_ref,
    moe_gain_ref,
    q_hbm,
    k_hbm,
    v_hbm,
    out_w_hbm,
    x_hbm,
    gate_hbm,
    up_hbm,
    down_hbm,
    common_gate_hbm,
    common_up_hbm,
    common_down_hbm,
    mixer_ref,
    experts_ref,
    x_v,
    normed,
    far_normed,
    far_ids,
    far_weight,
    chosen,
    packed,
    arrived,
    outs,
    returned,
    gate_v,
    up_v,
    down_v,
    act,
    hidden,
    common_gate,
    common_up,
    common_down,
    shared,
    part_out,
    part_in,
    q_v,
    k_v,
    v_v,
    rim_k,
    rim_v,
    out_w,
    mix,
    local_sems,
    send_sems,
    recv_sems,
    row_send,
    row_recv,
    ack_sem,
    *merge_refs,
):
    far = n_tp // PLANES
    tokens, d = x_v.shape
    top = ids_ref.shape[0]
    merging = bool(merge_refs)
    if merging:
        (
            home_ids,
            home_weight,
            home_chosen,
            home_rows,
            home_sums,
            home_out,
            home_in,
            meta_send,
            meta_recv,
            home_send,
            home_recv,
        ) = merge_refs
    slots = n_ep * cap
    width = gate_hbm.shape[1]
    half = far * width
    unit = d // sum(WIDTHS)
    me_e, me_t = lax.axis_index("ep"), lax.axis_index("tp")
    plane = me_t // far
    away = flip(me_t, far)
    mates = [flip(me_t, j) for j in range(1, far)]
    devices = n_ep * n_tp
    me = me_e * n_tp + me_t
    after, before = lax.rem(me + 1, devices), lax.rem(me + devices - 1, devices)
    local, net, shared_sends = Sems(local_sems), Sems(recv_sems), Sems(send_sems)

    line, spot = me_e // PAIR, lax.rem(me_e, PAIR)
    last = LINE - 1
    upper = line // (LINE // 2)
    home_line = last * (1 - upper)
    at_end = lax.rem(line, last) == 0
    end_flag = 1 - (lax.rem(line, last) + 1) // 2
    pair_e = line * PAIR + 1 - spot
    sent = {}

    def fetch(src, dst):
        copy = pltpu.make_async_copy(src, dst, local.take()[0])
        copy.start()
        return copy

    def remote(src, dst, e, t, name, start=True):
        if name not in sent:
            sent[name] = shared_sends.take()[0]
        copy = pltpu.make_async_remote_copy(
            src, dst, sent[name], net.take()[0], device_id=(e, t), device_id_type=MESH
        )
        if start:
            copy.start()
        return copy

    def settle(name, ref):
        pltpu.make_async_remote_copy(
            ref, ref, sent.pop(name), recv_sems.at[0], device_id=(me_e, away), device_id_type=MESH
        ).wait_send()

    def rows_of(group):
        return pl.ds(pl.multiple_of(group * cap, cap), cap)

    def exchange(phase, src, dst, cols, wanted=None, first=1, stride=1):
        def step(i, carry):
            j = first + stride * i
            to = lax.rem(me_e + j, n_ep)
            copy = pltpu.make_async_remote_copy(
                src.at[rows_of(to), cols],
                dst.at[rows_of(me_e), cols],
                row_send.at[min(phase, 2) // 2],
                row_recv.at[phase],
                device_id=(to, me_t),
                device_id_type=MESH,
            )
            if wanted is None:
                copy.start()
            else:
                pl.when(wanted(j))(lambda: copy.start())
            return carry

        lax.fori_loop(0, (n_ep - first + stride - 1) // stride, step, 0)

    def wait_rows(phase, dst, cols, peers):
        view = dst.at[pl.ds(0, peers * cap), cols]
        pltpu.make_async_remote_copy(
            view,
            view,
            row_send.at[0],
            row_recv.at[phase],
            device_id=(me_e, away),
            device_id_type=MESH,
        ).wait_recv()

    def wait_sent(kind, src, peers):
        view = src.at[:, pl.ds(0, peers * cap)]
        pltpu.make_async_remote_copy(
            view,
            view,
            row_send.at[kind],
            row_recv.at[0],
            device_id=(me_e, away),
            device_id_type=MESH,
        ).wait_send()

    def is_sent(j):
        return lax.rem(me_e + j, n_ep) // PAIR != home_line

    def keep_rows(src, dst, cols):
        dst[rows_of(me_e), cols] = src[rows_of(me_e), cols]

    everything = pl.ds(0, d)

    def wait_dispatch(side):
        wait_rows(side, arrived.at[side], everything, n_ep - 1)

    load_x = fetch(x_hbm, x_v)
    barrier = pltpu.get_barrier_semaphore()

    def greet(j, carry):
        pl.semaphore_signal(
            barrier, inc=1, device_id=(lax.rem(me_e + j, n_ep), me_t), device_id_type=MESH
        )
        return carry

    lax.fori_loop(1, n_ep, greet, 0)
    for t in [away] + mates:
        pl.semaphore_signal(barrier, inc=1, device_id=(me_e, t), device_id_type=MESH)
    for n in (after, before):
        pl.semaphore_signal(
            barrier, inc=1, device_id=(n // n_tp, lax.rem(n, n_tp)), device_id_type=MESH
        )
    if merging:
        pl.semaphore_signal(barrier, inc=1, device_id=(pair_e, away), device_id_type=MESH)
    own_loads = []
    for src, dst in ((gate_hbm, gate_v), (up_hbm, up_v), (down_hbm, down_v)):
        own_loads.append(fetch(src.at[plane], dst.at[0]))
    load_q = [fetch(q_hbm, q_v), fetch(k_hbm, k_v), fetch(v_hbm, v_v), fetch(out_w_hbm, out_w)]
    common_cols = common_gate_hbm.shape[1]
    common_loads = [
        fetch(common_gate_hbm, common_gate.at[:, pl.ds(0, common_cols)]),
        fetch(common_up_hbm, common_up.at[:, pl.ds(0, common_cols)]),
        fetch(common_down_hbm, common_down.at[pl.ds(0, common_cols)]),
    ]
    load_x.wait()
    normed[...] = rms_scale(x_v[...].astype(F32), pre_gain_ref[...]).astype(BF16)
    earlier = (iota((tokens, tokens), 0) < iota((tokens, tokens), 1)).astype(F32).astype(BF16)

    def route(ids, numbers, chosen_ref):
        hits = [numbers == ids[k : k + 1, :] for k in range(top)]
        hit = functools.reduce(lambda a, b: a | b, hits).astype(F32).astype(BF16)
        count = jnp.dot(hit, earlier, preferred_element_type=F32)
        place = count + (iota(numbers.shape, 0) * cap + 1).astype(F32)
        slot_number = (iota((chosen_ref.shape[0], tokens), 0) + 1).astype(F32)
        total = None
        for k in range(top):
            slot = jnp.sum(jnp.where(hits[k], place, 0.0), axis=0, keepdims=True)
            one_hot = (slot_number == slot).astype(F32).astype(BF16)
            chosen_ref[:, k * tokens : (k + 1) * tokens] = one_hot
            total = one_hot if total is None else total + one_hot
        return total

    def pack(ids, side, rows_ref):
        numbers = iota((n_ep, tokens), 0) * PLANES + plane
        one_hot = route(ids, numbers, chosen.at[side])
        rows = rows_ref[...]
        step = slots // 2
        for i in range(2):
            packed[side, i * step : (i + 1) * step, :] = jnp.dot(
                one_hot[i * step : (i + 1) * step], rows, preferred_element_type=F32
            ).astype(BF16)

    pack(ids_ref[...], 0, normed)
    pl.semaphore_wait(barrier, n_ep - 1 + far + 2 + int(merging))

    cut = width // 4
    first_rows, last_rows = pl.ds(0, cut), pl.ds(cut, width - cut)
    other = PLANES - 1 - plane
    gate_far = [
        remote(gate_hbm.at[other, first_rows], gate_v.at[far, first_rows], me_e, away, "gate"),
    ]
    meta = [
        remote(ids_ref, far_ids, me_e, away, "ids"),
        remote(weight_ref, far_weight, me_e, away, "weight"),
    ]
    mate_common, mate_kept = [], []
    for j, t in enumerate(mates, 1):
        cols = pl.ds(j * common_cols, common_cols)
        for kind, (src, dst) in enumerate(
            (
                (common_gate_hbm, common_gate.at[:, cols]),
                (common_up_hbm, common_up.at[:, cols]),
                (common_down_hbm, common_down.at[cols]),
            )
        ):
            mate_common.append(remote(src, dst, me_e, t, ("common", kind, j)))
    edge = k_hbm.shape[0] - WINDOW
    after_at = (after // n_tp, lax.rem(after, n_tp))
    rims = [
        remote(k_hbm.at[pl.ds(edge, WINDOW)], rim_k, *after_at, "rim_k", False),
        remote(v_hbm.at[pl.ds(edge, WINDOW)], rim_v, *after_at, "rim_v", False),
    ]

    def home_meta(n):
        lines = (LINE // 2 - upper, last - line)
        to = lines[n] * PAIR + spot
        return [
            pltpu.make_async_remote_copy(
                src,
                dst,
                meta_send.at[n, i],
                meta_recv.at[i],
                device_id=(to, me_t),
                device_id_type=MESH,
            )
            for i, (src, dst) in enumerate(((ids_ref, home_ids), (weight_ref, home_weight)))
        ]

    if merging:

        @pl.when(at_end)
        def _():
            for n in range(2):
                for copy in home_meta(n):
                    copy.start()

    normed_far = remote(normed, far_normed, me_e, away, "normed")
    gate_far.append(
        remote(gate_hbm.at[other, last_rows], gate_v.at[far, last_rows], me_e, away, "gate")
    )
    up_halves = [pl.ds(0, width // 2), pl.ds(width // 2, width // 2)]
    up_far = [
        remote(up_hbm.at[other, rows], up_v.at[far, rows], me_e, away, "up") for rows in up_halves
    ]
    chunks = [pl.ds(sum(WIDTHS[:c]) * unit, WIDTHS[c] * unit) for c in range(CHUNKS)]
    down_far = [
        remote(
            down_hbm.at[other, :, cols], down_v.at[far, :, cols], me_e, away, "down", c < AHEAD
        )
        for c, cols in enumerate(chunks)
    ]

    def dispatch(side):
        exchange(side, packed.at[side], arrived.at[side], everything)
        keep_rows(packed.at[side], arrived.at[side], everything)

    dispatch(0)
    for j, t in enumerate(mates, 1):
        for kind, (src, dst) in enumerate(
            ((gate_hbm, gate_v), (up_hbm, up_v), (down_hbm, down_v))
        ):
            mate_kept.append(remote(src.at[plane], dst.at[j], me_e, t, ("kept", kind, j)))

    group_size = HEADS // KV_HEADS
    blocks = q_v.shape[0] // WINDOW
    shape = (WINDOW, 2 * WINDOW)
    gap = iota(shape, 0) + WINDOW - iota(shape, 1)
    inside = (gap >= 0) & (gap < WINDOW)

    def attend(n):
        rows = pl.ds(n * WINDOW, WINDOW)
        valid = inside
        if n == 0:
            valid = inside & (iota(shape, 1) + me * q_v.shape[0] >= WINDOW)
        for g in range(KV_HEADS):
            cols = pl.ds(g * HEAD_DIM, HEAD_DIM)
            if n == 0:
                keys = jnp.concatenate([rim_k[:, cols], k_v[rows, cols]], axis=0)
                values = jnp.concatenate([rim_v[:, cols], v_v[rows, cols]], axis=0)
            else:
                band = pl.ds((n - 1) * WINDOW, 2 * WINDOW)
                keys, values = k_v[band, cols], v_v[band, cols]
            mixed = []
            for j in range(group_size):
                h = g * group_size + j
                query = q_v[rows, pl.ds(h * HEAD_DIM, HEAD_DIM)]
                scores = lax.dot_general(query, keys, NT, preferred_element_type=F32) * (
                    1.0 / math.sqrt(HEAD_DIM)
                )
                scores = jnp.where(valid, scores, NEGATIVE)
                sink = sink_ref[h]
                row_top = jnp.maximum(jnp.max(scores, axis=-1, keepdims=True), sink)
                weights = jnp.exp(scores - row_top)
                total = jnp.sum(weights, axis=-1, keepdims=True) + jnp.exp(sink - row_top)
                probs = (weights * (1.0 / total)).astype(BF16)
                mixed.append(jnp.dot(probs, values, preferred_element_type=F32).astype(BF16))
            span = group_size * HEAD_DIM
            mix[rows, pl.ds(g * span, span)] = jnp.concatenate(mixed, axis=1)

    def project(n):
        rows = pl.ds(n * WINDOW, WINDOW)
        projected = jnp.dot(mix[rows, :], out_w[...], preferred_element_type=F32)
        mixer_ref[rows, :] = rms_scale(projected, att_gain_ref[...]).astype(BF16)

    def relay(copy, view, kind):
        copy.wait_recv()
        return [
            remote(view(far), view(far + j), me_e, t, ("relay", kind, j))
            for j, t in enumerate(mates, 1)
        ]

    for load in load_q[:3]:
        load.wait()
    for n in range(1, blocks):
        attend(n)
    gate_mate = relay(gate_far[0], lambda b: gate_v.at[b, first_rows], 0)
    load_q[3].wait()
    for n in range(1, blocks):
        project(n)

    def attend_rim():
        for copy in rims:
            copy.wait_recv()
        before_at = (before // n_tp, lax.rem(before, n_tp))
        pl.semaphore_signal(ack_sem, inc=1, device_id=before_at, device_id_type=MESH)
        attend(0)
        project(0)

    def share(side, rows_ref):
        rows = rows_ref[...]
        gate = jnp.dot(rows, common_gate[...], preferred_element_type=F32)
        up = jnp.dot(rows, common_up[...], preferred_element_type=F32)
        units = (silu(gate) * up).astype(BF16)
        shared[side] = jnp.dot(units, common_down[...], preferred_element_type=F32)

    for load in common_loads:
        load.wait()
    for copy in mate_common:
        copy.wait_recv()
    share(0, normed)

    for copy in meta:
        copy.wait_recv()
    normed_far.wait_recv()
    pack(far_ids[...], 1, far_normed)
    dispatch(1)
    share(1, far_normed)

    if merging:
        block = iota((2 * PAIR, tokens), 0)
        over_y, over_x = block // 2, lax.rem(block, 2)
        group = line * PAIR + spot + over_y - 2 * spot * over_y
        for copy in home_meta(0):
            copy.wait_recv()
        route(
            home_ids[...], group * PLANES + plane + over_x - 2 * plane * over_x, home_chosen
        )

        @pl.when(at_end)
        def _():
            empty = pl.ds(pl.multiple_of((1 - upper) * (slots // 2), slots // 2), slots // 2)
            for side in range(2):
                returned[side, empty, :] = jnp.zeros((slots // 2, d), BF16)

    def product(side, weights, low, count):
        rows = arrived[side]
        matrix = weights[low : low + count].reshape(count * width, d)
        return lax.dot_general(rows, matrix, NT, preferred_element_type=F32)

    gate_mate += relay(gate_far[1], lambda b: gate_v.at[b, last_rows], 0)
    for load in own_loads:
        load.wait()
    for copy in mate_kept:
        copy.wait_recv()
    for copy in gate_mate:
        copy.wait_recv()
    wait_dispatch(0)
    act[0] = silu(product(0, gate_v, 0, 2 * far))
    hidden[0, :, :half] = (act[0, :, :half] * product(0, up_v, 0, far)).astype(BF16)
    up_mate = relay(up_far[0], lambda b: up_v.at[b, up_halves[0]], 1)
    up_mate += relay(up_far[1], lambda b: up_v.at[b, up_halves[1]], 1)
    wait_dispatch(1)
    act[1] = silu(product(1, gate_v, 0, 2 * far))
    hidden[1, :, :half] = (act[1, :, :half] * product(1, up_v, 0, far)).astype(BF16)

    def relay_down(c):
        cols = chunks[c]
        return relay(down_far[c], lambda b: down_v.at[b, :, cols], 2)

    down_mate = relay_down(0)
    for copy in up_mate:
        copy.wait_recv()
    for side in range(2):
        hidden[side, :, half:] = (act[side, :, half:] * product(side, up_v, far, far)).astype(BF16)

    def phase(side, c):
        return 2 + side * CHUNKS + c

    eye = iota((tokens, tokens), 0) == iota((tokens, tokens), 1)

    def columns_of(weights):
        return [
            jnp.sum(jnp.where(eye, weights[k : k + 1, :], 0.0), axis=1, keepdims=True)
            for k in range(top)
        ]

    def weigh(total, columns, one_hot, rows):
        picked = lax.dot_general(one_hot, rows, TN, preferred_element_type=F32)
        for k in range(top):
            part = columns[k] * picked[k * tokens : (k + 1) * tokens]
            total = part if total is None else total + part
        return total

    def home_blocks(c):
        routes = (
            (1, home_line * PAIR + spot, me_e, away),
            (0, home_line * PAIR + 1 - spot, pair_e, me_t),
            (1, home_line * PAIR + 1 - spot, pair_e, away),
        )
        return [
            pltpu.make_async_remote_copy(
                outs.at[side, rows_of(home), chunks[c]],
                home_rows.at[pl.ds(n * cap, cap), chunks[c]],
                home_send.at[1],
                home_recv.at[c, 1],
                device_id=(e, t),
                device_id_type=MESH,
            )
            for n, (side, home, e, t) in enumerate(routes, 1)
        ]

    def home_step(c):
        to = end_flag * (1 + line // last) + (1 - end_flag) * home_line
        return pltpu.make_async_remote_copy(
            home_out.at[:, chunks[c]],
            home_in.at[:, chunks[c]],
            home_send.at[0],
            home_recv.at[c, 0],
            device_id=(to * PAIR + spot, me_t),
            device_id_type=MESH,
        )

    def gather_home(c):
        for copy in home_blocks(c):
            copy.start()
        home_rows[0:cap, chunks[c]] = outs[0, rows_of(home_line * PAIR + spot), chunks[c]]

    def sum_home(c):
        view = home_rows.at[pl.ds(0, (2 * PAIR - 1) * cap), chunks[c]]
        pltpu.make_async_remote_copy(
            view,
            view,
            home_send.at[1],
            home_recv.at[c, 1],
            device_id=(me_e, away),
            device_id_type=MESH,
        ).wait_recv()
        sums = weigh(None, home_columns, home_chosen[...], home_rows[:, chunks[c]])

        @pl.when(at_end)
        def _():
            home_out[:, chunks[c]] = sums.astype(BF16)
            home_step(c).start()

        @pl.when(jnp.logical_not(at_end))
        def _():
            home_sums[:, chunks[c]] = sums

    def pass_home(c):
        @pl.when(jnp.logical_not(at_end))
        def _():
            home_step(c).wait_recv()
            sums = home_sums[:, chunks[c]] + home_in[:, chunks[c]].astype(F32)
            home_out[:, chunks[c]] = sums.astype(BF16)
            home_step(c).start()

    if merging:
        home_columns = columns_of(home_weight[...])

    def send_back(side, c, first):
        exchange(
            phase(side, c),
            outs.at[side],
            returned.at[side],
            chunks[c],
            is_sent if merging else None,
            first,
            2,
        )

    for c, cols in enumerate(chunks):
        if c:
            down_mate = relay_down(c)
        for copy in down_mate:
            copy.wait_recv()
        matrix = down_v[:, :, cols].reshape(2 * half, WIDTHS[c] * unit)
        for side in range(2):
            outs[side, :, cols] = jnp.dot(hidden[side], matrix, preferred_element_type=F32).astype(BF16)
        if merging:
            gather_home(c)
        if c + AHEAD < CHUNKS:
            down_far[c + AHEAD].start()
        if c + AHEAD == CHUNKS:
            for copy in rims:
                copy.start()
        if merging:
            if c:
                sum_home(c - 1)
            if c == CHUNKS - 1:
                sum_home(c)
        for side in (1, 0):
            if side or c <= EARLY:
                send_back(side, c, 2)
            if c < EARLY:
                send_back(side, c, 1)
            keep_rows(outs.at[side], returned.at[side], cols)
        if merging and c >= 2:
            pass_home(c - 2)
    for c in range(EARLY, CHUNKS):
        send_back(1, c, 1)

    scales = [columns_of(weight_ref[...]), columns_of(far_weight[...])]

    def wait_back(side, c):
        if not merging:
            wait_rows(phase(side, c), returned.at[side], chunks[c], n_ep - 1)
            return

        @pl.when(at_end)
        def _():
            wait_rows(phase(side, c), returned.at[side], chunks[c], n_ep // 2 - 1)

        @pl.when(jnp.logical_not(at_end))
        def _():
            wait_rows(phase(side, c), returned.at[side], chunks[c], n_ep - 1)

    def combine(side, c):
        wait_back(side, c)
        cols = chunks[c]
        return weigh(shared[side, :, cols], scales[side], chosen[side], returned[side, :, cols])

    parts = []

    def combine_far(c):
        cols = chunks[c]
        part_out[:, cols] = combine(1, c).astype(BF16)
        parts.append(remote(part_out.at[:, cols], part_in.at[:, cols], me_e, away, "part"))

    def combine_own(c):
        shared[0, :, chunks[c]] = combine(0, c)

    for c in range(EARLY):
        combine_far(c)
    if merging:
        pass_home(CHUNKS - 2)
    for c in range(EARLY):
        combine_own(c)
    if merging:
        pass_home(CHUNKS - 1)
    for c in range(EARLY, CHUNKS):
        if c > EARLY:
            send_back(0, c, 2)
        send_back(0, c, 1)
    attend_rim()
    for c in range(EARLY, CHUNKS):
        combine_far(c)
    for c in range(EARLY, CHUNKS):
        combine_own(c)

    wait_sent(0, packed, n_ep - 1)
    wait_sent(1, outs, n_ep - 1 - (PAIR if merging else 0))
    settle("ids", ids_ref)
    settle("weight", weight_ref)
    settle("normed", normed)
    settle("rim_k", rim_k)
    settle("rim_v", rim_v)
    for name, ref in (("gate", gate_hbm), ("up", up_hbm), ("down", down_hbm)):
        settle(name, ref.at[other])
    for j in range(1, far):
        for kind, ref in enumerate((gate_v, up_v, down_v)):
            settle(("kept", kind, j), ref.at[0])
            settle(("relay", kind, j), ref.at[far])
        for kind, ref in enumerate((common_gate_hbm, common_up_hbm, common_down_hbm)):
            settle(("common", kind, j), ref)
    if merging:
        for n, view in enumerate((home_out, home_rows.at[pl.ds(0, (2 * PAIR - 1) * cap)])):
            pltpu.make_async_remote_copy(
                view,
                view,
                home_send.at[n],
                home_recv.at[0, 0],
                device_id=(me_e, away),
                device_id_type=MESH,
            ).wait_send()
    pl.semaphore_wait(ack_sem, 1)
    if merging:

        @pl.when(at_end)
        def _():
            for n in range(2):
                for copy in home_meta(n):
                    copy.wait_send()

    square = jnp.zeros((tokens, 1), F32)
    for c, cols in enumerate(chunks):
        if merging:

            @pl.when(at_end)
            def _():
                home_step(c).wait_recv()
                shared[0, :, cols] += home_in[:, cols].astype(F32)

        parts[c].wait_recv()
        total = shared[0, :, cols] + part_in[:, cols].astype(F32)
        shared[0, :, cols] = total
        square = square + jnp.sum(total * total, axis=-1, keepdims=True)
    scale = lax.rsqrt(square * (1.0 / d) + EPS)
    experts_ref[...] = (shared[0] * scale * moe_gain_ref[...]).astype(BF16)
    settle("part", part_out)
    assert not sent


def body(
    att_queries,
    att_keys,
    att_values,
    sink_logits,
    out_weight,
    att_gain,
    moe_in,
    pre_gain,
    expert_ids,
    routed_expert_weight,
    w_gate,
    w_up,
    w_down,
    common_expert_gate_weight,
    common_expert_up_weight,
    common_expert_down_weight,
    moe_gain,
):
    assert w_gate.shape[0] == PLANES
    n_ep, n_tp = lax.axis_size("ep"), lax.axis_size("tp")
    rows, width = att_queries.shape
    tokens, d = moe_in.shape
    top = expert_ids.shape[1]
    slot_cap = 2 * tokens * top // (PLANES * n_ep)
    cap = -(-slot_cap // ROW_TILE) * ROW_TILE
    slots = cap * n_ep
    far = n_tp // PLANES
    blocks = 2 * far
    kv = att_keys.shape[1]
    units = w_gate.shape[2]
    common = common_expert_gate_weight.shape[1]
    scratch = [
        pltpu.VMEM((tokens, d), BF16),
        pltpu.VMEM((tokens, d), BF16),
        pltpu.VMEM((tokens, d), BF16),
        pltpu.VMEM((top, tokens), jnp.int32),
        pltpu.VMEM((top, tokens), F32),
        pltpu.VMEM((2, slots, top * tokens), BF16),
        pltpu.VMEM((2, slots, d), BF16),
        pltpu.VMEM((2, slots, d), BF16),
        pltpu.VMEM((2, slots, d), BF16),
        pltpu.VMEM((2, slots, d), BF16),
        pltpu.VMEM((blocks, units, d), BF16),
        pltpu.VMEM((blocks, units, d), BF16),
        pltpu.VMEM((blocks, units, d), BF16),
        pltpu.VMEM((2, slots, blocks * units), F32),
        pltpu.VMEM((2, slots, blocks * units), BF16),
        pltpu.VMEM((d, far * common), BF16),
        pltpu.VMEM((d, far * common), BF16),
        pltpu.VMEM((far * common, d), BF16),
        pltpu.VMEM((2, tokens, d), F32),
        pltpu.VMEM((tokens, d), BF16),
        pltpu.VMEM((tokens, d), BF16),
        pltpu.VMEM((rows, width), BF16),
        pltpu.VMEM((rows, kv), BF16),
        pltpu.VMEM((rows, kv), BF16),
        pltpu.VMEM((WINDOW, kv), BF16),
        pltpu.VMEM((WINDOW, kv), BF16),
        pltpu.VMEM(out_weight.shape, BF16),
        pltpu.VMEM((rows, width), BF16),
        pltpu.SemaphoreType.DMA((11,)),
        pltpu.SemaphoreType.DMA((9 + (far - 1) * 9,)),
        pltpu.SemaphoreType.DMA((9 + 2 * CHUNKS + (far - 1) * (10 + CHUNKS),)),
        pltpu.SemaphoreType.DMA((2,)),
        pltpu.SemaphoreType.DMA((2 + 2 * CHUNKS,)),
        pltpu.SemaphoreType.REGULAR,
    ]
    if n_ep == PAIR * LINE and far == 2:
        scratch += [
            pltpu.VMEM((top, tokens), jnp.int32),
            pltpu.VMEM((top, tokens), F32),
            pltpu.VMEM((2 * PAIR * cap, top * tokens), BF16),
            pltpu.VMEM((2 * PAIR * cap, d), BF16),
            pltpu.VMEM((tokens, d), F32),
            pltpu.VMEM((tokens, d), BF16),
            pltpu.VMEM((tokens, d), BF16),
            pltpu.SemaphoreType.DMA((2, 2)),
            pltpu.SemaphoreType.DMA((2,)),
            pltpu.SemaphoreType.DMA((2,)),
            pltpu.SemaphoreType.DMA((CHUNKS, 2)),
        ]
    return pl.pallas_call(
        functools.partial(layer_kernel, n_ep, n_tp, cap),
        out_shape=(
            pltpu.VMEM((rows, d), BF16),
            pltpu.VMEM((tokens, d), BF16),
        ),
        in_specs=[SMEM] + [VMEM] * 5 + [ANY] * 11,
        out_specs=(VMEM, VMEM),
        scratch_shapes=scratch,
        compiler_params=pltpu.CompilerParams(
            vmem_limit_bytes=62 * 1024 * 1024 + 256 * 1024, collective_id=0, has_side_effects=True
        ),
        name="layer",
    )(
        sink_logits,
        expert_ids.T,
        routed_expert_weight.T,
        pre_gain[None],
        att_gain[None],
        moe_gain[None],
        att_queries,
        att_keys,
        att_values,
        out_weight,
        moe_in,
        jnp.swapaxes(w_gate, 1, 2),
        jnp.swapaxes(w_up, 1, 2),
        w_down,
        common_expert_gate_weight,
        common_expert_up_weight,
        common_expert_down_weight,
    )


def solution(mesh):
    tokens_spec = P(("ep", "tp"), None)
    in_specs = (
        tokens_spec,
        tokens_spec,
        tokens_spec,
        P(),
        P(),
        P(),
        tokens_spec,
        P(),
        tokens_spec,
        tokens_spec,
        P("ep", None, "tp"),
        P("ep", None, "tp"),
        P("ep", "tp", None),
        P(None, "tp"),
        P(None, "tp"),
        P("tp", None),
        P(),
    )
    return jax.shard_map(
        body, mesh=mesh, in_specs=in_specs, out_specs=(tokens_spec, tokens_spec), check_vma=False
    )
```
